256 devices in a mesh: ep: 64 (over z, y, core), tp: 4 (over x).
Axes of the slice: x: 4, y: 4, z: 8, core: 2. Of those that a mesh axis runs over, the one named last changes fastest.
Arguments:
- tokens: bfloat16 [1024, 4096], P(None, 'ep'), may hold values from -80 to 80
- mix_gain: bfloat16 [4096], P('ep'), may hold values from 0.099609375 to 1.8984375
- w_query: bfloat16 [4096, 1024], P('ep', 'tp'), may hold values from -0.09375 to 0.09375
- w_key: bfloat16 [4096, 1024], P('ep', 'tp'), may hold values from -0.09375 to 0.09375
- w_value: bfloat16 [4096, 2048], P('ep', 'tp'), may hold values from -0.09375 to 0.09375
- w_outgate: bfloat16 [4096, 2048], P('ep', 'tp'), may hold values from -0.09375 to 0.09375
- w_igate: bfloat16 [4096, 16], P('ep', 'tp'), may hold values from -0.09375 to 0.09375
- w_fgate: bfloat16 [4096, 16], P('ep', 'tp'), may hold values from -0.09375 to 0.09375
- igate_bias: float32 [16], P('tp'), may hold values from -3 to 3
- fgate_bias: float32 [16], P('tp'), may hold values from -1 to 3
- head_gain: bfloat16 [2048], P('tp'), may hold values from 0.099609375 to 1.8984375
- w_mixout: bfloat16 [2048, 4096], P('tp', 'ep'), may hold values from -0.125 to 0.125
- state_matrix: float32 [1024, 16, 64, 128], P('ep', 'tp'), may hold values from -3 to 3
- state_norm: float32 [1024, 16, 64], P('ep', 'tp'), may hold values from -3 to 3
- state_max: float32 [1024, 16], P('ep', 'tp'), may hold values from -3 to 3
- ffn_gain: bfloat16 [4096], P('ep'), may hold values from 0.099609375 to 1.8984375
- dense_mix: bfloat16 [4096], P('ep'), may hold values from -0.09375 to 0.09375
- w_dense_gate: bfloat16 [4096, 1024], P('ep', 'tp'), may hold values from -0.09375 to 0.09375
- w_dense_up: bfloat16 [4096, 1024], P('ep', 'tp'), may hold values from -0.09375 to 0.09375
- w_dense_down: bfloat16 [1024, 4096], P('tp', 'ep'), may hold values from -0.1875 to 0.1875
- routes: int32 [1024, 4], replicated, may hold values from 0 to 63, all different within a row; in each aligned block of 16 rows (0 to 15, 16 to 31, ...) at most 2 rows name the same one
- route_weights: float32 [1024, 4], replicated, may hold values from 0.2 to 1.5
- w_exp_gate: bfloat16 [64, 4096, 1024], P('ep', None, 'tp'), may hold values from -0.09375 to 0.09375
- w_exp_up: bfloat16 [64, 4096, 1024], P('ep', None, 'tp'), may hold values from -0.09375 to 0.09375
- w_exp_down: bfloat16 [64, 1024, 4096], P('ep', 'tp'), may hold values from -0.1875 to 0.1875
Outputs:
- layer_out: bfloat16 [1024, 4096], P(None, 'ep')
- new_matrix: float32 [1024, 16, 64, 128], P('ep', 'tp')
- new_norm: float32 [1024, 16, 64], P('ep', 'tp')
- new_max: float32 [1024, 16], P('ep', 'tp')
The draws below stay inside these ranges and needn't reach their ends.
Inputs may be any that keep to these rules, and one draw needn't show every extreme that they name: `routes`: each row names 4 different experts. In the rows of one device (aligned blocks of 16 rows) no expert is named by more than 2 rows, a bound that some block reaches.
All inputs are finite; a program needn't handle non-finite values.
Results may differ from the reference program's by a relative error of at most 0.012.
Values may be sent and summed in bfloat16 or wider, within the bound.
A program may use at most 128 MiB of HBM per device.

```python
import math
import jax
import jax.numpy as jnp
import numpy as np
from jax import lax

D = 4096
H = 16
DK = 64
DV = 128
FE = 1024
FS = 1024
TOPK = 4
SEQ_DEV = 16
HQK = 1024
HV = 2048
EXPERTS = 64
BATCH = 1024
CAP = 2
UNIT_GROUP = 256
N_EP = 64
N_TP = 4


def draw_tokens(key, part):
    base_key, scale_key, column_key = jax.random.split(key, 3)
    noise = jnp.clip(jax.random.normal(base_key, (BATCH, D), jnp.float32), -5.0, 5.0)
    row_scale = jnp.exp(jax.random.uniform(scale_key, (BATCH, 1), jnp.float32, math.log(0.4), math.log(2.5)))
    col_scale = 3.0 ** (jnp.arange(D, dtype=jnp.float32) / D) * jnp.exp(jax.random.uniform(column_key, (D,), jnp.float32, -0.35, 0.35))
    return (noise * row_scale * col_scale[None, :]).astype(jnp.bfloat16)


def level_of(rng, extent, cuts, least, top_value):
    loudness = 1.0
    for axis_at, blocks in cuts:
        steps = jax.random.uniform(jax.random.fold_in(jax.random.fold_in(rng, 6), axis_at), (blocks,), jnp.float32, least / len(cuts), top_value / len(cuts))
        loudness = loudness * jnp.repeat(jnp.exp(steps), extent[axis_at] // blocks).reshape((-1,) + (1,) * (len(extent) - 1 - axis_at))
    return loudness


def deal_out(rng, own, number, rows, amount, top, limit, lean):
    sequence = jax.random.permutation(rng, amount)
    heavy_load, common = load_shares(amount, rows * top, limit, lean, True), load_shares(amount, rows * top, limit, lean, False)
    places = jnp.arange(amount)

    def named(sizes, offset_by):
        used = int((sizes > 0).sum())
        fixed = max(1, used // 4)
        passed = fixed + (places - fixed + offset_by * (used - fixed)) % max(1, amount - fixed)
        return jnp.zeros((amount,), jnp.int32).at[sequence[jnp.where(places < fixed, places, passed)]].set(jnp.asarray(sizes, jnp.int32))

    sizes = jnp.where(number % 4 == 0, named(heavy_load, number // 4), named(common, number - number // 4 - 1))
    mixed = jax.random.permutation(jax.random.fold_in(own, 3), amount)
    source_of, receiver = mixed[0:amount // 2 * 2:2], mixed[1:amount // 2 * 2:2]
    room = jnp.minimum(sizes[source_of] - 1, limit - sizes[receiver]) // 2
    room = jnp.where((source_of == sequence[0]) | (receiver == sequence[0]) | (sizes[receiver] == 0), 0, jnp.maximum(room, 0))
    passed = jax.random.randint(jax.random.fold_in(own, 4), (amount // 2,), 0, 1 << 20) % (room + 1)
    sizes = sizes.at[source_of].add(-passed).at[receiver].add(passed)
    labels = jnp.searchsorted(jnp.cumsum(sizes), jnp.arange(rows * top), side="right").astype(jnp.int32)
    table = labels.reshape(top, rows).T
    table = table[jax.random.permutation(jax.random.fold_in(own, 1), rows)]
    offset_by = jax.random.randint(jax.random.fold_in(own, 2), (rows, 1), 0, top)
    return jnp.take_along_axis(table, (jnp.arange(top)[None, :] + offset_by) % top, axis=1)


def load_shares(count, total, bound, lean, full):
    weights = [(1 << 20) // math.isqrt(grade ** lean) + 1 for grade in range(1, count + 1)]
    largest = bound if full else min(bound, max(-(-total // count), total * weights[0] // sum(weights)))
    least = 1 if total - largest >= count - 1 else 0
    given, spare = [largest] + [least] * (count - 1), total - largest - least * (count - 1)
    while spare > 0:
        candidates = [i for i in range(1, count) if given[i] < largest] or [i for i in range(1, count) if given[i] < bound]
        whole, remaining = sum([weights[i] for i in candidates]), spare
        for i in candidates:
            extra = min(bound - given[i], max(1, remaining * weights[i] // whole), spare)
            given[i] = given[i] + extra
            spare = spare - extra
    return np.array(given)


def scatter_about(stream_key, shape, scale, reach, pieces=(), kind=jnp.bfloat16):
    array = scale * jax.random.normal(stream_key, shape, jnp.float32)
    if pieces:
        array = array * level_of(stream_key, shape, pieces, -0.22, 0.18)
    return jnp.clip(array, -reach, reach).astype(kind)


def setup_inputs(seed: int = 0) -> dict:
    keys = jax.random.split(jax.random.key(seed), 26)
    tokens = draw_tokens(jax.random.fold_in(keys[25], 71), 0)
    mix_gain = jnp.clip(1.0 + 0.18 * jax.random.normal(keys[1], (D,), jnp.float32), 0.099609375, 1.8984375).astype(jnp.bfloat16)
    w_query = scatter_about(keys[2], (D, HQK), D ** -0.5, 0.09375, ((0, 64), (1, 4)))
    w_key = scatter_about(keys[3], (D, HQK), D ** -0.5, 0.09375, ((0, 64), (1, 4)))
    w_value = scatter_about(keys[4], (D, HV), D ** -0.5, 0.09375, ((0, 64), (1, 4)))
    w_outgate = scatter_about(keys[5], (D, HV), D ** -0.5, 0.09375, ((0, 64), (1, 4)))
    w_igate = scatter_about(keys[6], (D, H), D ** -0.5, 0.09375, ((0, 64), (1, 4)))
    w_fgate = scatter_about(keys[7], (D, H), D ** -0.5, 0.09375, ((0, 64), (1, 4)))
    igate_bias = scatter_about(keys[8], (H,), 1.0, 3.0, ((0, 4),), jnp.float32)
    fgate_bias = jnp.clip(-1.0 + 4.0 * jax.random.uniform(keys[9], (H,), jnp.float32) ** level_of(keys[9], (H,), ((0, 4),), -0.2, 0.2), -1.0, 3.0)
    head_gain = jnp.clip(1.0 + 0.18 * jax.random.normal(keys[10], (HV,), jnp.float32), 0.099609375, 1.8984375).astype(jnp.bfloat16)
    w_mixout = scatter_about(keys[11], (HV, D), HV ** -0.5, 0.125, ((0, 4), (1, 64)))
    state_matrix = scatter_about(keys[12], (BATCH, H, DK, DV), 0.5, 3.0, ((0, 64), (1, 4)), jnp.float32)
    state_norm = scatter_about(keys[13], (BATCH, H, DK), 0.5, 3.0, ((0, 64), (1, 4)), jnp.float32)
    state_max = scatter_about(keys[14], (BATCH, H), 1.0, 3.0, ((0, 64), (1, 4)), jnp.float32)
    ffn_gain = jnp.clip(1.0 + 0.18 * jax.random.normal(keys[15], (D,), jnp.float32), 0.099609375, 1.8984375).astype(jnp.bfloat16)
    dense_mix = scatter_about(keys[16], (D,), D ** -0.5, 0.09375, ((0, 64),))
    w_dense_gate = scatter_about(keys[17], (D, FS), D ** -0.5, 0.09375, ((0, 64), (1, 4)))
    w_dense_up = scatter_about(keys[18], (D, FS), D ** -0.5, 0.09375, ((0, 64), (1, 4)))
    w_dense_down = scatter_about(keys[19], (FS, D), FS ** -0.5, 0.1875, ((0, 4), (1, 64)))
    routes_keys = jax.random.split(jax.random.fold_in(keys[20], 1), BATCH // SEQ_DEV)
    routes_turns = jax.random.permutation(jax.random.fold_in(keys[20], 3), BATCH // SEQ_DEV)
    routes = jax.vmap(lambda own, number: deal_out(jax.random.fold_in(keys[20], 2), own, number, SEQ_DEV, EXPERTS, TOPK, CAP, 2))(routes_keys, routes_turns).reshape((BATCH, TOPK))
    route_weights = jnp.clip(jnp.exp(jax.random.uniform(keys[21], (BATCH, TOPK), jnp.float32, math.log(0.2), math.log(1.5))), 0.2, 1.5)
    w_exp_gate = scatter_about(keys[22], (EXPERTS, D, FE), D ** -0.5, 0.09375, ((0, 64), (2, 4)))
    w_exp_up = scatter_about(keys[23], (EXPERTS, D, FE), D ** -0.5, 0.09375, ((0, 64), (2, 4)))
    w_exp_down = scatter_about(keys[24], (EXPERTS, FE, D), FE ** -0.5, 0.1875, ((0, 64), (1, 4)))
    return dict(tokens=tokens, mix_gain=mix_gain, w_query=w_query, w_key=w_key, w_value=w_value, w_outgate=w_outgate, w_igate=w_igate, w_fgate=w_fgate, igate_bias=igate_bias, fgate_bias=fgate_bias, head_gain=head_gain, w_mixout=w_mixout, state_matrix=state_matrix, state_norm=state_norm, state_max=state_max, ffn_gain=ffn_gain, dense_mix=dense_mix, w_dense_gate=w_dense_gate, w_dense_up=w_dense_up, w_dense_down=w_dense_down, routes=routes, route_weights=route_weights, w_exp_gate=w_exp_gate, w_exp_up=w_exp_up, w_exp_down=w_exp_down)


EPSILON = 1e-06
SOFT_CAP = 15.0

def gate_logs(in_pre, forget_pre, igate_bias, fgate_bias):
    in_log = SOFT_CAP * jnp.tanh((in_pre + igate_bias) / SOFT_CAP)
    forget_log = jax.nn.log_sigmoid(SOFT_CAP * jnp.tanh((forget_pre + fgate_bias) / SOFT_CAP))
    return (in_log, forget_log)

def recurrent_read(queries, keys_in, values_in, in_log, forget_log, state_matrix, state_norm, state_max):
    scaled_query = queries.astype(jnp.float32) * queries.shape[-1] ** (-0.5)
    key_float = keys_in.astype(jnp.float32)
    value_float = values_in.astype(jnp.float32)
    new_max = jnp.maximum(forget_log + state_max, in_log)
    carried = jnp.exp(forget_log + state_max - new_max)
    fresh_weight = jnp.exp(in_log - new_max)
    new_matrix = carried[..., None, None] * state_matrix + fresh_weight[..., None, None] * key_float[..., :, None] * value_float[..., None, :]
    new_norm = carried[..., None] * state_norm + fresh_weight[..., None] * key_float
    numerator = lax.optimization_barrier(jnp.sum(new_matrix * scaled_query[..., :, None], axis=-2))
    denominator = lax.optimization_barrier(jnp.sum(new_norm * scaled_query, axis=-1))
    floor_value = jnp.maximum(jnp.abs(denominator), jnp.exp(-new_max))
    readout = numerator / floor_value[..., None]
    return (readout, new_matrix, new_norm, new_max)

def head_output(readout, outgates, head_gain):
    scaled = readout * lax.rsqrt(lax.optimization_barrier(jnp.mean(readout * readout, axis=-1, keepdims=True)) + EPSILON)
    rows_count, heads_count, head_width = readout.shape
    gated_rows = scaled.reshape(rows_count, heads_count * head_width) * head_gain.astype(jnp.float32)[None, :]
    gated_rows = gated_rows * jax.nn.sigmoid(outgates.astype(jnp.float32))
    return gated_rows.astype(jnp.bfloat16)

def expert_slots(routes, groups, capacity, experts_all):
    row_total = routes.shape[0]
    chosen = (routes[:, :, None] == jnp.arange(experts_all, dtype=jnp.int32)[None, None, :]).astype(jnp.int32)
    per_row = lax.optimization_barrier(jnp.sum(chosen, axis=1))
    grouped = per_row.reshape(groups, row_total // groups, experts_all)
    earlier = (jnp.cumsum(grouped, axis=1) - grouped).reshape(row_total, experts_all)
    rank_in = lax.optimization_barrier(jnp.sum(chosen * earlier[:, None, :], axis=2))
    group_of = jnp.arange(row_total, dtype=jnp.int32) // (row_total // groups)
    return (routes * (groups * capacity) + group_of[:, None] * capacity + rank_in).astype(jnp.int32)

def reference(tokens, mix_gain, w_query, w_key, w_value, w_outgate, w_igate, w_fgate, igate_bias, fgate_bias, head_gain, w_mixout, state_matrix, state_norm, state_max, ffn_gain, dense_mix, w_dense_gate, w_dense_up, w_dense_down, routes, route_weights, w_exp_gate, w_exp_up, w_exp_down):
    token_float = tokens.astype(jnp.float32)
    inverse = lax.rsqrt(lax.optimization_barrier(jnp.mean(token_float * token_float, axis=1)) + EPSILON)
    normed = (token_float * inverse[:, None] * mix_gain.astype(jnp.float32)[None, :]).astype(jnp.bfloat16)
    queries = jnp.dot(normed, w_query, preferred_element_type=jnp.float32).astype(jnp.bfloat16).reshape(BATCH, H, DK)
    keys_in = jnp.dot(normed, w_key, preferred_element_type=jnp.float32).astype(jnp.bfloat16).reshape(BATCH, H, DK)
    values_in = jnp.dot(normed, w_value, preferred_element_type=jnp.float32).astype(jnp.bfloat16).reshape(BATCH, H, DV)
    outgates = jnp.dot(normed, w_outgate, preferred_element_type=jnp.float32).astype(jnp.bfloat16)
    in_pre = jnp.dot(normed, w_igate, preferred_element_type=jnp.float32)
    forget_pre = jnp.dot(normed, w_fgate, preferred_element_type=jnp.float32)
    in_log, forget_log = gate_logs(in_pre, forget_pre, igate_bias, fgate_bias)
    readout, new_matrix, new_norm, new_max = recurrent_read(queries, keys_in, values_in, in_log, forget_log, state_matrix, state_norm, state_max)
    heads_out = head_output(readout, outgates, head_gain)
    mixer = lax.optimization_barrier(jnp.dot(heads_out, w_mixout, preferred_element_type=jnp.float32).astype(jnp.bfloat16))
    hidden_state = lax.optimization_barrier((token_float + mixer.astype(jnp.float32)).astype(jnp.bfloat16))
    hidden_float = hidden_state.astype(jnp.float32)
    gain_float = ffn_gain.astype(jnp.float32)
    inverse_two = lax.rsqrt(lax.optimization_barrier(jnp.mean(hidden_float * hidden_float, axis=1)) + EPSILON)
    dense_gate = inverse_two * lax.optimization_barrier(jnp.sum(hidden_float * gain_float[None, :] * dense_mix.astype(jnp.float32)[None, :], axis=1))
    normed_two = (hidden_float * inverse_two[:, None] * gain_float[None, :]).astype(jnp.bfloat16)
    dense_hidden = (jax.nn.silu(jnp.dot(normed_two, w_dense_gate, preferred_element_type=jnp.float32)) * jnp.dot(normed_two, w_dense_up, preferred_element_type=jnp.float32)).astype(jnp.bfloat16)
    dense = jnp.dot(dense_hidden, w_dense_down, preferred_element_type=jnp.float32)
    flat_index = expert_slots(routes, N_EP, CAP, EXPERTS).reshape(-1)
    slot_count = N_EP * CAP
    send_rows = jnp.zeros((EXPERTS * slot_count, D), jnp.bfloat16).at[flat_index].set(jnp.repeat(normed_two, TOPK, axis=0)).reshape(EXPERTS, slot_count, D)

    def run_expert(operands):
        gate_matrix, up_matrix, down_matrix, arrived = operands
        gate_part = jnp.dot(arrived, gate_matrix, preferred_element_type=jnp.float32)
        up_part = jnp.dot(arrived, up_matrix, preferred_element_type=jnp.float32)
        expert_hidden = (jax.nn.silu(gate_part) * up_part).astype(jnp.bfloat16)
        summed = jnp.zeros((arrived.shape[0], D), jnp.float32)
        for group_index in range(N_TP):
            lower = group_index * UNIT_GROUP
            expert_part = jnp.dot(expert_hidden[:, lower:lower + UNIT_GROUP], down_matrix[lower:lower + UNIT_GROUP], preferred_element_type=jnp.float32).astype(jnp.bfloat16)
            summed = summed + lax.optimization_barrier(expert_part).astype(jnp.float32)
        return summed
    returned = lax.map(run_expert, (w_exp_gate, w_exp_up, w_exp_down, send_rows))
    picked = returned.reshape(EXPERTS * slot_count, D)[flat_index].reshape(BATCH, TOPK, D)
    routed = lax.optimization_barrier(jnp.sum(picked * route_weights[:, :, None], axis=1))
    layer_out = (hidden_float + routed + jax.nn.sigmoid(dense_gate)[:, None] * dense).astype(jnp.bfloat16)
    return (layer_out, new_matrix, new_norm, new_max)
```

```python
import jax
import jax.numpy as jnp
from jax import lax
from jax.experimental import pallas as pl
from jax.experimental.pallas import tpu as pltpu
from jax.sharding import PartitionSpec as P

D = 4096
EPSILON = 1e-06
SOFT_CAP = 15.0
BF, F32 = jnp.bfloat16, jnp.float32
MESH = pl.DeviceIdType.MESH


def rem(a, n):
    return lax.rem(a, jnp.int32(n))


def div(a, n):
    return lax.div(a, jnp.int32(n))


def coords():
    e, x = lax.axis_index("ep"), lax.axis_index("tp")
    return div(e, 8), div(rem(e, 8), 2), rem(e, 2), x


class Net:
    def __init__(self, ssem, rsem, lsem):
        self.ssem, self.rsem, self.lsem = ssem, rsem, lsem
        self.at, self.lat = 0, 0
        self.open = []
        self.z, self.y, self.c, self.x = coords()

    def dev(self, dz=0, dy=0, dc=0, dx=0):
        z = rem(self.z + dz, 8) if dz else self.z
        y = rem(self.y + dy, 4) if dy else self.y
        c = 1 - self.c if dc else self.c
        x = rem(self.x + dx, 4) if dx else self.x
        return {"ep": z * 8 + y * 2 + c, "tp": x}

    def enter(self, peers):
        barrier = pltpu.get_barrier_semaphore()
        for p in peers:
            pl.semaphore_signal(barrier, inc=1, device_id=self.dev(**p), device_id_type=MESH)
        pl.semaphore_wait(barrier, len(peers))

    def send(self, src, dst, **peer):
        copy = pltpu.make_async_remote_copy(
            src_ref=src,
            dst_ref=dst,
            send_sem=self.ssem.at[self.at],
            recv_sem=self.rsem.at[self.at],
            device_id=self.dev(**peer),
            device_id_type=MESH,
        )
        self.at += 1
        copy.start()
        self.open.append(copy)
        return copy

    def local(self, src, dst):
        copy = pltpu.make_async_copy(src, dst, self.lsem.at[self.lat])
        self.lat += 1
        copy.start()
        return copy

    def got(self, copy):
        copy.wait_recv()
        copy.got = True

    def finish(self):
        for copy in self.open:
            if not getattr(copy, "got", False):
                copy.wait_recv()
        for copy in self.open:
            copy.wait_send()


def exchange(body, ins, outs, scratch, copies, cid):
    vmem = pl.BlockSpec(memory_space=pltpu.VMEM)
    return pl.pallas_call(
        body,
        out_shape=[jax.ShapeDtypeStruct(s, t) for s, t in outs],
        in_specs=[vmem] * len(ins),
        out_specs=[vmem] * len(outs),
        scratch_shapes=[pltpu.VMEM(s, t) for s, t in scratch]
        + [
            pltpu.SemaphoreType.DMA((copies,)),
            pltpu.SemaphoreType.DMA((copies,)),
            pltpu.SemaphoreType.DMA((8,)),
        ],
        compiler_params=pltpu.CompilerParams(
            collective_id=cid, has_side_effects=True, vmem_limit_bytes=32 * 1024 * 1024
        ),
        name=body.__name__,
    )(*ins)


YC = [dict(dy=dy, dc=dc) for dy in range(4) for dc in range(2) if dy or dc]
ZS = [1, 7, 2, 6, 3, 5, 4]
ZP = [dict(dz=d) for d in ZS]
YP = [dict(dy=d) for d in (1, 3, 2)]
XP = [dict(dx=d) for d in (1, 3, 2)]


def ex_first(W, T, S, G, PR, DG, Wg, Tg, Sg, Gg, Pg, Dg, ssem, rsem, lsem):
    n = Net(ssem, rsem, lsem)
    j = n.y * 2 + n.c
    n.enter(YC)
    up = n.send(W, Wg.at[j], dy=1)
    down = n.send(W, Wg.at[j], dy=3)
    for p in YC:
        to = rem(n.y + p["dy"], 4) * 2 + (1 - n.c if p["dc"] else n.c)
        n.send(T.at[to], Tg.at[j], **p)
        n.send(S.at[to], Sg.at[j], **p)
        n.send(G, Gg.at[j], **p)
    n.send(W, Wg.at[j], dc=1)
    n.send(PR, Pg, dc=1)
    n.send(DG, Dg, dc=1)
    Wg[j] = W[...]
    Tg[j] = T[j]
    Sg[j] = S[j]
    Gg[j] = G[...]
    below = rem(n.y + 3, 4) * 2 + n.c
    above = rem(n.y + 1, 4) * 2 + n.c
    far = rem(n.y + 2, 4) * 2 + n.c
    half = Wg.shape[1] // 2
    n.got(up)
    first = n.send(Wg.at[below, pl.ds(0, half)], Wg.at[below, pl.ds(0, half)], dy=1)
    n.send(Wg.at[below], Wg.at[below], dc=1)
    n.got(down)
    second = n.send(Wg.at[above, pl.ds(half, half)], Wg.at[above, pl.ds(half, half)], dy=3)
    n.send(Wg.at[above], Wg.at[above], dc=1)
    n.got(first)
    n.got(second)
    n.send(Wg.at[far], Wg.at[far], dc=1)
    n.finish()


def ex_rows(M, E, G, Mg, Eg, Gg, ssem, rsem, lsem):
    n = Net(ssem, rsem, lsem)
    n.enter(ZP)
    for d in ZS:
        to = rem(n.z + d, 8)
        n.send(M.at[to], Mg.at[n.z], dz=d)
        n.send(E.at[to], Eg.at[n.z], dz=d)
    for d in ZS:
        n.send(G, Gg.at[n.z], dz=d)
    Mg[n.z] = M[n.z]
    Eg[n.z] = E[n.z]
    Gg[n.z] = G[...]
    n.finish()


UPWARD = (0, 1, 2, 4)


def zy_gather(n, src, dst):
    dst[n.z, n.y] = src[...]
    zc = {d: n.send(src, dst.at[n.z, n.y], dz=d) for d in ZS}
    order = [0] + ZS
    ups, downs = {}, {}
    for d in order:
        if d:
            n.got(zc[d])
            piece = dst.at[rem(n.z + 8 - d, 8), n.y]
        else:
            piece = src
        there = dst.at[rem(n.z + 8 - d, 8), n.y]
        ups[d] = n.send(piece, there, dy=1)
        downs[d] = n.send(piece, there, dy=3)
    for d in order:
        zs = rem(n.z + 8 - d, 8)
        if d in UPWARD:
            n.got(ups[d])
            piece = dst.at[zs, rem(n.y + 3, 4)]
            n.send(piece, piece, dy=1)
        else:
            n.got(downs[d])
            piece = dst.at[zs, rem(n.y + 1, 4)]
            n.send(piece, piece, dy=3)


def ex_heads(Hd, Hg, ssem, rsem, lsem):
    n = Net(ssem, rsem, lsem)
    n.enter(ZP + YP)
    zy_gather(n, Hd, Hg)
    n.finish()


def ex_mixer(M, Mg, ssem, rsem, lsem):
    n = Net(ssem, rsem, lsem)
    n.enter(XP)
    half = M.shape[0] // 2
    up = n.send(M, Mg.at[n.x], dx=1)
    down = n.send(M, Mg.at[n.x], dx=3)
    Mg[n.x] = M[...]
    below, above = rem(n.x + 3, 4), rem(n.x + 1, 4)
    n.got(up)
    n.send(Mg.at[below, pl.ds(0, half)], Mg.at[below, pl.ds(0, half)], dx=1)
    n.got(down)
    n.send(Mg.at[above, pl.ds(half, half)], Mg.at[above, pl.ds(half, half)], dx=3)
    n.finish()


def ex_dispatch(S, Pd, Gx, B2, A, A2, ssem, rsem, lsem):
    n = Net(ssem, rsem, lsem)
    n.enter(ZP + YC + XP)
    j = n.y * 2 + n.c
    own = n.local(S.at[n.z], A.at[n.z])
    own2 = n.local(Pd.at[n.z], A2.at[n.z])
    zc = [n.send(S.at[rem(n.z + d, 8)], A.at[n.z], dz=d) for d in ZS]
    zd = [n.send(Pd.at[rem(n.z + d, 8)], A2.at[n.z], dz=d) for d in ZS]
    own.wait()
    for copy in zc:
        n.got(copy)
    mine = n.local(A.at[:, j], Gx.at[n.x, :, j])
    yc = []
    for p in YC:
        to = rem(n.y + p["dy"], 4) * 2 + (1 - n.c if p["dc"] else n.c)
        yc.append(n.send(A.at[:, to], Gx.at[n.x, :, j], **p))
    mine.wait()
    ups, downs = [], []
    for i in range(8):
        if i:
            n.got(yc[i - 1])
            p = YC[i - 1]
            jj = rem(n.y + 4 - p["dy"], 4) * 2 + (1 - n.c if p["dc"] else n.c)
        else:
            jj = j
        piece = Gx.at[n.x, :, jj]
        ups.append((n.send(piece, piece, dx=1), jj))
        downs.append((n.send(piece, piece, dx=3), jj))
    own2.wait()
    for copy in zd:
        n.got(copy)
    for p in YP:
        n.send(A2.at[:, rem(n.y + p["dy"], 4)], B2.at[n.y], **p)
    B2[n.y] = A2[:, n.y]
    for i in range(8):
        if i < 4:
            copy, jj = ups[i]
            n.got(copy)
            piece = Gx.at[rem(n.x + 3, 4), :, jj]
            n.send(piece, piece, dx=1)
        else:
            copy, jj = downs[i]
            n.got(copy)
            piece = Gx.at[rem(n.x + 1, 4), :, jj]
            n.send(piece, piece, dx=3)
    n.finish()


def ex_hidden(O, Hd, Og, Hg, ssem, rsem, lsem):
    n = Net(ssem, rsem, lsem)
    n.enter(ZP + YP + XP)
    for p in XP:
        n.send(O.at[rem(n.x + p["dx"], 4)], Og.at[n.x], **p)
    zy_gather(n, Hd, Hg)
    Og[n.x] = O[n.x]
    n.finish()


def ex_return(R, Dp, B, Dq, A, ssem, rsem, lsem):
    n = Net(ssem, rsem, lsem)
    n.enter(ZP + YC + XP)
    j = n.y * 2 + n.c
    own = n.local(R.at[n.z], A.at[n.z])
    zc = [n.send(R.at[rem(n.z + d, 8)], A.at[n.z], dz=d) for d in ZS]
    for p in XP:
        n.send(Dp.at[rem(n.x + p["dx"], 4)], Dq.at[n.x], **p)
    Dq[n.x] = Dp[n.x]
    own.wait()
    for copy in zc:
        n.got(copy)
    for p in YC:
        to = rem(n.y + p["dy"], 4) * 2 + (1 - n.c if p["dc"] else n.c)
        n.send(A.at[:, to], B.at[:, j], **p)
    B[:, j] = A[:, j]
    n.finish()


def ex_final(M, Fo, ssem, rsem, lsem):
    n = Net(ssem, rsem, lsem)
    n.enter(XP + [dict(dc=1)])
    cs = [n.send(M, Fo.at[n.c, n.x], **p) for p in XP]
    n.send(M, Fo.at[n.c, n.x], dc=1)
    Fo[n.c, n.x] = M[...]
    for p, copy in zip(XP, cs):
        n.got(copy)
        piece = Fo.at[n.c, rem(n.x + 4 - p["dx"], 4)]
        n.send(piece, piece, dc=1)
    n.finish()


def plain(body, ins, outs, grid=None, in_specs=None, out_specs=None, scratch=(), flops=10**6):
    vmem = pl.BlockSpec(memory_space=pltpu.VMEM)
    kw = {}
    if grid is not None:
        kw = dict(grid=grid)
    return pl.pallas_call(
        body,
        out_shape=[jax.ShapeDtypeStruct(s, t) for s, t in outs],
        in_specs=in_specs or [vmem] * len(ins),
        out_specs=out_specs or [vmem] * len(outs),
        scratch_shapes=[pltpu.VMEM(s, t) for s, t in scratch],
        compiler_params=pltpu.CompilerParams(vmem_limit_bytes=40 * 1024 * 1024),
        name=body.__name__,
        **kw,
    )(*ins)


def mm_first(Tg, Wg, Sg, M, E):
    a = Tg[...].reshape(512, 128).T
    ss = jnp.sum(Sg[...], axis=0)
    sst = jnp.concatenate([ss, jnp.zeros((120, 128), F32)], axis=0).T
    for at in range(0, 1536, 512):
        w = Wg[:, :, at : at + 512].reshape(512, 512)
        M[:, :, at : at + 512] = (
            jnp.dot(a, w, preferred_element_type=F32).astype(BF).reshape(8, 16, 512)
        )
    w = Wg[:, :, 1536:1664].reshape(512, 128)
    E[...] = (jnp.dot(a, w, preferred_element_type=F32) + sst).reshape(8, 16, 128)


def log_sigmoid(v):
    return jnp.minimum(v, 0.0) - jnp.log1p(jnp.exp(-jnp.abs(v)))


def cell(Mg, Eg, GB, SM, HG, SN, ST, NM, NN, NX, HO, qt, kt, vv, cc, oo, num, dn):
    step = pl.program_id(0)

    @pl.when(step == 0)
    def _():
        acc = jnp.sum(Mg[...].astype(F32), axis=0)
        ext = jnp.sum(Eg[...], axis=0)
        inv = lax.rsqrt(ext[:, 0:1] * (1.0 / D) + EPSILON)
        proj = (acc * inv).astype(BF).astype(F32)
        pre = ext * inv
        in_log = SOFT_CAP * jnp.tanh((pre + GB[0:1, :]) / SOFT_CAP)
        forget = pltpu.roll(pre, 124, 1)
        forget_log = log_sigmoid(SOFT_CAP * jnp.tanh((forget + GB[1:2, :]) / SOFT_CAP))
        smax = SM[...]
        new_max = jnp.maximum(forget_log + smax, in_log)
        carried = jnp.exp(forget_log + smax - new_max)
        fresh = jnp.exp(in_log - new_max)
        floor = jnp.exp(-new_max)
        NX[...] = new_max
        cc[...] = carried
        q = proj[:, 0:256] * 0.125
        k = proj[:, 256:512]
        vv[...] = proj[:, 512:1024]
        oo[...] = proj[:, 1024:1536]
        fk = []
        for h in range(4):
            lane = slice(8 + h, 9 + h)
            kh = k[:, h * 64 : (h + 1) * 64] * fresh[:, lane]
            qh = q[:, h * 64 : (h + 1) * 64]
            nn = carried[:, lane] * SN[:, h, :] + kh
            NN[:, h, :] = nn
            den = jnp.sum(nn * qh, axis=1, keepdims=True)
            dn[:, h * 128 : (h + 1) * 128] = jnp.broadcast_to(
                jnp.maximum(jnp.abs(den), floor[:, lane]), (16, 128)
            )
            fk.append(kh)
        fk = jnp.concatenate(fk, axis=1)
        zeros = jnp.zeros((112, 256), F32)
        qt[...] = jnp.concatenate([q, zeros], axis=0).T
        kt[...] = jnp.concatenate([fk, zeros], axis=0).T

    shift = rem(128 - step * 4, 128)
    qr = pltpu.roll(qt[...], shift, 1)
    kr = pltpu.roll(kt[...], shift, 1)
    for r in range(4):
        row = step * 4 + r
        crow = cc[pl.ds(row, 1), :]
        vrow = vv[pl.ds(row, 1), :]
        for h in range(4):
            qc = jnp.broadcast_to(qr[h * 64 : (h + 1) * 64, r : r + 1], (64, 128))
            kc = jnp.broadcast_to(kr[h * 64 : (h + 1) * 64, r : r + 1], (64, 128))
            new = crow[:, 8 + h : 9 + h] * ST[r, h] + kc * vrow[:, h * 128 : (h + 1) * 128]
            NM[r, h] = new
            num[row, :, h * 128 : (h + 1) * 128] = jnp.sum(new * qc, axis=0, keepdims=True)

    @pl.when(step == 3)
    def _():
        read = jnp.concatenate([num[i] for i in range(16)], axis=0) / dn[...]
        parts = []
        for h in range(4):
            rh = read[:, h * 128 : (h + 1) * 128]
            parts.append(
                rh * lax.rsqrt(jnp.mean(rh * rh, axis=1, keepdims=True) + EPSILON)
            )
        scaled = jnp.concatenate(parts, axis=1) * HG[...].astype(F32)
        HO[...] = (scaled / (1.0 + jnp.exp(-oo[...]))).astype(BF)


def run_cell(mg, eg, gb, sm, hg, sn, st):
    full = lambda s: pl.BlockSpec(s, lambda i: (0,) * len(s))
    state = pl.BlockSpec((4, 4, 64, 128), lambda i: (i, 0, 0, 0))
    return plain(
        cell,
        (mg, eg, gb, sm, hg, sn, st),
        [((16, 4, 64, 128), F32), ((16, 4, 64), F32), ((16, 128), F32), ((16, 512), BF)],
        grid=(4,),
        in_specs=[
            full((8, 16, 1536)),
            full((8, 16, 128)),
            full((8, 128)),
            full((16, 128)),
            full((1, 512)),
            full((16, 4, 64)),
            state,
        ],
        out_specs=[state, full((16, 4, 64)), full((16, 128)), full((16, 512))],
        scratch=[
            ((256, 128), F32),
            ((256, 128), F32),
            ((16, 512), F32),
            ((16, 128), F32),
            ((16, 512), F32),
            ((16, 1, 512), F32),
            ((16, 512), F32),
        ],
    )


def mm_mixer(Hg, PO, PG, M):
    w = PO[0:512] + PG[0:512]
    M[...] = jnp.dot(Hg[...].reshape(512, 512), w, preferred_element_type=F32).astype(BF)


def high_low(v):
    high = v.astype(BF)
    return high, (v - high.astype(F32)).astype(BF)


def spread(X, Mg, TO, PG, GV, DO, DG, Dm, S, Pd, Hq, hs):
    mixer = jnp.sum(Mg[...].astype(F32), axis=0).astype(BF)
    token = TO[...].astype(F32) + PG[...].astype(F32)
    hb = (token + mixer.astype(F32)).astype(BF)
    h = hb.astype(F32)
    hs[...] = h
    gain, mix = GV[0:1, :], GV[1:2, :]
    hg = h * gain
    ss = jnp.sum(h * h, axis=1, keepdims=True)
    gd = jnp.sum(hg * mix, axis=1, keepdims=True)
    prod = hg.astype(BF)
    first = DG[0]
    c_is = X[1]
    w0 = jnp.where(c_is == 0, DO[...], first)
    w1 = jnp.where(c_is == 0, first, DO[...])
    w = jnp.concatenate([w0, w1], axis=0)
    Pd[:, :, :, 0:512] = (
        jnp.dot(prod, w, preferred_element_type=F32).astype(BF).reshape(8, 4, 16, 512)
    )
    lane = lax.broadcasted_iota(jnp.int32, (512, 128), 1)
    sh = ss.astype(BF).astype(F32)
    gh = gd.astype(BF).astype(F32)
    cols = jnp.where(
        lane == 0,
        sh,
        jnp.where(lane == 1, ss - sh, jnp.where(lane == 2, gh, jnp.where(lane == 3, gd - gh, 0.0))),
    )
    Pd[:, :, :, 512:640] = cols.astype(BF).reshape(8, 4, 16, 128)
    hq = hs[pl.ds(pl.multiple_of(X[0] * 128, 128), 128), :].astype(BF)
    Hq[...] = hq
    S[...] = jnp.dot(Dm[...], hq, preferred_element_type=F32).astype(BF).reshape(8, 8, 16, 128)


def ffn(Gx, GA, WG, WU, WD, O, ga, ua, sq):
    step = pl.program_id(0)

    @pl.when(step == 0)
    def _():
        ga[...] = jnp.zeros_like(ga)
        ua[...] = jnp.zeros_like(ua)
        sq[...] = jnp.zeros_like(sq)

    parts = []
    s2 = sq[...]
    for y in range(4):
        block = Gx[:, 0, 2 * y : 2 * y + 2].reshape(128, 128).astype(F32)
        s2 = s2 + block * block
        gain = GA[0, 2 * y, 0:1, :] + GA[0, 2 * y + 1, 0:1, :]
        parts.append((block * gain).astype(BF))
    sq[...] = s2
    rows = jnp.concatenate(parts, axis=1)
    ga[...] += jnp.dot(rows, WG[0], preferred_element_type=F32)
    ua[...] += jnp.dot(rows, WU[0], preferred_element_type=F32)

    @pl.when(step == 7)
    def _():
        inv = lax.rsqrt(jnp.sum(sq[...], axis=1, keepdims=True) * (1.0 / D) + EPSILON)
        g = ga[...] * inv
        u = ua[...] * inv
        hid = (g / (1.0 + jnp.exp(-g)) * u).astype(BF)

        def out(zy, carry):
            at = pl.multiple_of(zy * 512, 512)
            res = jnp.dot(hid, WD[0, :, pl.ds(at, 512)], preferred_element_type=F32).astype(BF)
            for y in range(4):
                for c in range(2):
                    for x in range(4):
                        O[x, zy, 2 * y + c] = res[
                            (x * 2 + c) * 16 : (x * 2 + c + 1) * 16, y * 128 : (y + 1) * 128
                        ]
            return carry

        lax.fori_loop(0, 8, out, 0)


def run_ffn(gx, gall, wg, wu, wd):
    full = lambda s: pl.BlockSpec(s, lambda i: (0,) * len(s))
    return plain(
        ffn,
        (gx, gall, wg, wu, wd),
        [((4, 8, 8, 16, 128), BF)],
        grid=(8,),
        in_specs=[
            pl.BlockSpec((4, 1, 8, 16, 128), lambda i: (0, i, 0, 0, 0)),
            pl.BlockSpec((1, 8, 8, 128), lambda i: (i, 0, 0, 0)),
            pl.BlockSpec((1, 512, 256), lambda i: (0, i, 0)),
            pl.BlockSpec((1, 512, 256), lambda i: (0, i, 0)),
            full((1, 256, 4096)),
        ],
        out_specs=[full((4, 8, 8, 16, 128))],
        scratch=[((128, 256), F32), ((128, 256), F32), ((128, 128), F32)],
    )[0]


def dense_mid(B2, Hd):
    s = jnp.sum(B2[...].reshape(32, 16, 640).astype(F32), axis=0)
    ext = s[:, 512:640]
    ss = ext[:, 0:1] + ext[:, 1:2]
    gd = ext[:, 2:3] + ext[:, 3:4]
    inv = lax.rsqrt(ss * (1.0 / D) + EPSILON)
    gate = inv * gd
    g = s[:, 0:256] * inv
    u = s[:, 256:512] * inv
    Hd[...] = (g / (1.0 + jnp.exp(-g)) * u / (1.0 + jnp.exp(-gate))).astype(BF)


def reduce_mid(Og, Hg, DO, DP, R, Dp):
    for z in range(8):
        R[z] = jnp.sum(Og[:, z].astype(F32), axis=0).astype(BF)
    w = DO[...] + DP[...]
    Dp[...] = (
        jnp.dot(Hg[...].reshape(512, 256), w, preferred_element_type=F32)
        .astype(BF)
        .reshape(4, 128, 128)
    )


def combine(B, Dh, Dl, Dq, Hq, out):
    got = B[...].reshape(1024, 128)
    routed = jnp.dot(Dh[...], got, preferred_element_type=F32)
    routed += jnp.dot(Dl[...], got, preferred_element_type=F32)
    dense = jnp.sum(Dq[...].astype(F32), axis=0)
    out[...] = (Hq[...].astype(F32) + routed + dense).astype(BF)


def on_device(
    tokens,
    mix_gain,
    w_query,
    w_key,
    w_value,
    w_outgate,
    w_igate,
    w_fgate,
    igate_bias,
    fgate_bias,
    head_gain,
    w_mixout,
    state_matrix,
    state_norm,
    state_max,
    ffn_gain,
    dense_mix,
    w_dense_gate,
    w_dense_up,
    w_dense_down,
    routes,
    route_weights,
    w_exp_gate,
    w_exp_up,
    w_exp_down,
):
    z, y, c, x = coords()

    def half(v):
        wide = jnp.zeros(v.shape, v.dtype)
        return jnp.where(
            c == 0, jnp.concatenate([v, wide], axis=-1), jnp.concatenate([wide, v], axis=-1)
        )

    token_float = tokens.astype(F32)
    gained = (token_float * mix_gain.astype(F32)[None, :]).astype(BF)
    T = gained.reshape(8, 8, 16, 64).transpose(1, 3, 0, 2).reshape(8, 64, 128)
    squares = jnp.sum(token_float * token_float, axis=1).reshape(8, 8, 16).transpose(1, 0, 2)
    S = jnp.pad(squares.reshape(8, 1, 128), ((0, 0), (0, 7), (0, 0)))
    W = jnp.concatenate(
        [
            w_query,
            w_key,
            w_value,
            w_outgate,
            jnp.zeros((64, 8), BF),
            w_igate,
            w_fgate,
            jnp.zeros((64, 112), BF),
        ],
        axis=1,
    )
    G = half(jnp.stack([ffn_gain.astype(F32), dense_mix.astype(F32)]))
    G = jnp.pad(G, ((0, 6), (0, 0)))
    by_core = tokens.reshape(8, 4, 2, 16, 64)
    tok_own = half(lax.dynamic_index_in_dim(by_core, c, 2, False).reshape(512, 64))
    tok_far = half(lax.dynamic_index_in_dim(by_core, 1 - c, 2, False).reshape(512, 64))
    mix_own = half(w_mixout)
    down_own = half(w_dense_down)
    dgu = jnp.concatenate([w_dense_gate, w_dense_up], axis=1)
    pair = jnp.concatenate([mix_own, tok_far, down_own], axis=0)

    r4 = lax.dynamic_index_in_dim(
        lax.dynamic_index_in_dim(routes.reshape(4, 2, 4, 2, 16, 4), x, 0, False), c, 2, False
    ).reshape(128, 4)
    w4 = lax.dynamic_index_in_dim(
        lax.dynamic_index_in_dim(route_weights.reshape(4, 2, 4, 2, 16, 4), x, 0, False), c, 2, False
    ).reshape(128, 4)
    hit = r4[None, :, :] == jnp.arange(64, dtype=jnp.int32)[:, None, None]
    picked = jnp.any(hit, axis=2)
    weight = jnp.sum(jnp.where(hit, w4[None], 0.0), axis=2)
    rows = jnp.arange(128, dtype=jnp.int32)
    earlier = (rows[:, None] // 16 == rows[None, :] // 16) & (rows[:, None] < rows[None, :])
    rank = jnp.dot(picked.astype(BF), earlier.astype(BF), preferred_element_type=F32)
    slot = jnp.arange(16, dtype=jnp.int32)
    fits = slot[:, None] // 2 == rows[None, :] // 16
    taken = (
        picked[:, None, :]
        & (rank[:, None, :] == (slot % 2).astype(F32)[None, :, None])
        & fits[None]
    ).reshape(1024, 128)
    Dm = taken.astype(BF)
    weighted = jnp.where(
        taken, jnp.broadcast_to(weight[:, None, :], (64, 16, 128)).reshape(1024, 128), 0.0
    ).T
    Dh, Dl = high_low(weighted)

    Wg, Tg, Sg, Gg, Pg, Dg = exchange(
        ex_first,
        (W, T, S, G, pair, dgu),
        [
            ((8, 64, 1664), BF),
            ((8, 64, 128), BF),
            ((8, 8, 128), F32),
            ((8, 8, 128), F32),
            ((1280, 128), BF),
            ((64, 512), BF),
        ],
        [],
        32,
        0,
    )
    M, E = plain(mm_first, (Tg, Wg, Sg), [((8, 16, 1536), BF), ((8, 16, 128), F32)])
    Mg, Eg, GA = exchange(
        ex_rows,
        (M, E, Gg),
        [((8, 16, 1536), BF), ((8, 16, 128), F32), ((8, 8, 8, 128), F32)],
        [],
        21,
        1,
    )
    gb = jnp.stack([igate_bias, fgate_bias])
    gb = jnp.pad(gb, ((0, 6), (8, 116)))
    sm = jnp.pad(state_max, ((0, 0), (8, 116)))
    new_matrix, new_norm, nx, heads = run_cell(
        Mg, Eg, gb, sm, head_gain[None, :], state_norm, state_matrix
    )
    new_max = nx[:, 8:12]
    (Hg,) = exchange(ex_heads, (heads,), [((8, 4, 16, 512), BF)], [], 31, 2)
    (mx,) = plain(mm_mixer, (Hg, mix_own, Pg), [((512, 128), BF)])
    (Mx,) = exchange(ex_mixer, (mx,), [((4, 512, 128), BF)], [], 4, 3)

    GV = lax.dynamic_slice_in_dim(Gg, y * 2, 2, 0).sum(axis=0)
    where = jnp.stack([x, c])
    vmem = pl.BlockSpec(memory_space=pltpu.VMEM)
    slots, Pd, hq = plain(
        spread,
        (where, Mx, tok_own, Pg[512:1024], GV, dgu, Dg[None], Dm),
        [((8, 8, 16, 128), BF), ((8, 4, 16, 640), BF), ((128, 128), BF)],
        in_specs=[pl.BlockSpec(memory_space=pltpu.SMEM)] + [vmem] * 7,
        scratch=[((512, 128), F32)],
    )
    Gx, B2 = exchange(
        ex_dispatch,
        (slots, Pd),
        [((4, 8, 8, 16, 128), BF), ((4, 8, 16, 640), BF)],
        [((8, 8, 16, 128), BF), ((8, 4, 16, 640), BF)],
        48,
        4,
    )
    (hidden,) = plain(dense_mid, (B2,), [((16, 256), BF)])
    O = run_ffn(Gx, GA, w_exp_gate, w_exp_up, w_exp_down)
    Og, Hd = exchange(
        ex_hidden, (O, hidden), [((4, 8, 8, 16, 128), BF), ((8, 4, 16, 256), BF)], [], 34, 5
    )
    R, Dp = plain(
        reduce_mid,
        (Og, Hd, down_own, Pg[1024:1280]),
        [((8, 8, 16, 128), BF), ((4, 128, 128), BF)],
    )
    B, Dq = exchange(
        ex_return,
        (R, Dp),
        [((8, 8, 16, 128), BF), ((4, 128, 128), BF)],
        [((8, 8, 16, 128), BF)],
        17,
        6,
    )
    (rows_out,) = plain(combine, (B, Dh, Dl, Dq, hq), [((128, 128), BF)])
    (Fo,) = exchange(ex_final, (rows_out,), [((2, 4, 128, 128), BF)], [], 7, 7)
    both = Fo.reshape(2, 32, 16, 128)
    mine = jnp.where(c == 0, both[..., :64], both[..., 64:])
    layer_out = mine.transpose(1, 0, 2, 3).reshape(1024, 64)
    return (layer_out, new_matrix, new_norm, new_max)


def solution(mesh):
    return jax.shard_map(
        on_device,
        mesh=mesh,
        in_specs=(
            P(None, "ep"),
            P("ep"),
            P("ep", "tp"),
            P("ep", "tp"),
            P("ep", "tp"),
            P("ep", "tp"),
            P("ep", "tp"),
            P("ep", "tp"),
            P("tp"),
            P("tp"),
            P("tp"),
            P("tp", "ep"),
            P("ep", "tp", None, None),
            P("ep", "tp", None),
            P("ep", "tp"),
            P("ep"),
            P("ep"),
            P("ep", "tp"),
            P("ep", "tp"),
            P("tp", "ep"),
            P(),
            P(),
            P("ep", None, "tp"),
            P("ep", None, "tp"),
            P("ep", "tp", None),
        ),
        out_specs=(P(None, "ep"), P("ep", "tp", None, None), P("ep", "tp", None), P("ep", "tp")),
        check_vma=False,
    )
```

```python
import jax
import jax.numpy as jnp
from jax import lax
from jax.experimental import pallas as pl
from jax.experimental.pallas import tpu as pltpu
from jax.sharding import PartitionSpec as P

D = 4096
EPSILON = 1e-06
SOFT_CAP = 15.0
BF, F32 = jnp.bfloat16, jnp.float32
MESH = pl.DeviceIdType.MESH


def rem(a, n):
    return lax.rem(a, jnp.int32(n))


def div(a, n):
    return lax.div(a, jnp.int32(n))


def coords():
    e, x = lax.axis_index("ep"), lax.axis_index("tp")
    return div(e, 8), div(rem(e, 8), 2), rem(e, 2), x


class Net:
    def __init__(self, ssem, rsem, lsem):
        self.ssem, self.rsem, self.lsem = ssem, rsem, lsem
        self.at, self.lat = 0, 0
        self.open = []
        self.z, self.y, self.c, self.x = coords()

    def dev(self, dz=0, dy=0, dc=0, dx=0):
        z = rem(self.z + dz, 8) if dz else self.z
        y = rem(self.y + dy, 4) if dy else self.y
        c = 1 - self.c if dc else self.c
        x = rem(self.x + dx, 4) if dx else self.x
        return {"ep": z * 8 + y * 2 + c, "tp": x}

    def enter(self, peers):
        barrier = pltpu.get_barrier_semaphore()
        for p in peers:
            pl.semaphore_signal(barrier, inc=1, device_id=self.dev(**p), device_id_type=MESH)
        pl.semaphore_wait(barrier, len(peers))

    def send(self, src, dst, **peer):
        copy = pltpu.make_async_remote_copy(
            src_ref=src,
            dst_ref=dst,
            send_sem=self.ssem.at[self.at],
            recv_sem=self.rsem.at[self.at],
            device_id=self.dev(**peer),
            device_id_type=MESH,
        )
        self.at += 1
        copy.start()
        self.open.append(copy)
        return copy

    def local(self, src, dst):
        copy = pltpu.make_async_copy(src, dst, self.lsem.at[self.lat])
        self.lat += 1
        copy.start()
        return copy

    def got(self, copy):
        copy.wait_recv()
        copy.got = True

    def flush(self):
        for copy in self.open:
            if not getattr(copy, "got", False):
                self.got(copy)

    def finish(self):
        self.flush()
        for copy in self.open:
            copy.wait_send()


def exchange(body, ins, outs, scratch, copies, cid):
    vmem = pl.BlockSpec(memory_space=pltpu.VMEM)
    return pl.pallas_call(
        body,
        out_shape=[jax.ShapeDtypeStruct(s, t) for s, t in outs],
        in_specs=[vmem] * len(ins),
        out_specs=[vmem] * len(outs),
        scratch_shapes=[pltpu.VMEM(s, t) for s, t in scratch]
        + [
            pltpu.SemaphoreType.DMA((copies,)),
            pltpu.SemaphoreType.DMA((copies,)),
            pltpu.SemaphoreType.DMA((8,)),
        ],
        compiler_params=pltpu.CompilerParams(
            collective_id=cid, has_side_effects=True, vmem_limit_bytes=32 * 1024 * 1024
        ),
        name=body.__name__,
    )(*ins)


YC = [dict(dy=dy, dc=dc) for dy in range(4) for dc in range(2) if dy or dc]
ZS = [1, 7, 2, 6, 3, 5, 4]
ZP = [dict(dz=d) for d in ZS]
YP = [dict(dy=d) for d in (1, 3, 2)]
XP = [dict(dx=d) for d in (1, 3, 2)]


UPWARD = (0, 1, 2, 4)


def core_of(n, p):
    return 1 - n.c if p["dc"] else n.c


def project(W, T, S, G, PR, DG, Mg, GA, Pg, Dg, Wg, Tg, Sg, Gg, M, Gz, ssem, rsem, lsem):
    n = Net(ssem, rsem, lsem)
    j = n.y * 2 + n.c
    n.enter(YC + ZP)
    small = []
    for p in YC:
        to = rem(n.y + p["dy"], 4) * 2 + core_of(n, p)
        small.append(n.send(T.at[to], Tg.at[j], **p))
        small.append(n.send(S.at[to], Sg.at[j], **p))
    spans = [pl.ds(0, 640), pl.ds(640, 512), pl.ds(1152, 512)]
    ys, cs = [], []
    for ch in spans:
        cs.append([n.send(W.at[:, ch], Wg.at[j, :, ch], dc=1)])
        ys.append([n.send(W.at[:, ch], Wg.at[j, :, ch], **p) for p in YP])
    gs = [n.send(G, Gg.at[j], **p) for p in YC]
    n.send(PR, Pg, dc=1)
    n.send(DG, Dg, dc=1)
    Wg[j] = W[...]
    Tg[j] = T[j]
    Sg[j] = S[j]
    Gg[j] = G[...]
    a = None
    for i, ch in enumerate(spans):
        for p, copy in zip(YP, ys[i]):
            n.got(copy)
            piece = Wg.at[rem(n.y + 4 - p["dy"], 4) * 2 + n.c, :, ch]
            cs[i].append(n.send(piece, piece, dc=1))
        if i == 0:
            for copy in small:
                n.got(copy)
            a = Tg[...].reshape(512, 128).T
        for copy in cs[i]:
            n.got(copy)
        w = Wg[:, :, ch].reshape(512, ch.size)
        res = jnp.dot(a, w, preferred_element_type=F32)
        if i == 0:
            ss = jnp.sum(Sg[...], axis=0)
            ext = res[:, 0:128] + jnp.concatenate([ss, jnp.zeros((120, 128), F32)], axis=0).T
            high = ext.astype(BF).astype(F32)
            ext = high + pltpu.roll(ext - high, 64, 1)
            M[:, :, 0:128] = ext.astype(BF).reshape(8, 16, 128)
            M[:, :, 128:640] = res[:, 128:].astype(BF).reshape(8, 16, 512)
        else:
            M[:, :, ch] = res.astype(BF).reshape(8, 16, 512)
        for d in ZS:
            n.send(M.at[rem(n.z + d, 8), :, ch], Mg.at[n.z, :, ch], dz=d)
    for copy in gs:
        n.got(copy)
    Gz[...] = jnp.sum(Gg[...], axis=0)
    for d in ZS:
        n.send(Gz, GA.at[n.z], dz=d)
    GA[n.z] = Gz[...]
    Mg[n.z] = M[n.z]
    n.finish()


class Gather:
    def __init__(self, n, src, dst):
        self.n, self.src, self.dst = n, src, dst
        self.zc = {d: n.send(src, dst.at[n.z, n.y], dz=d) for d in ZS}
        dst[n.z, n.y] = src[...]
        self.ups, self.downs = {}, {}

    def onward(self, order):
        n, dst = self.n, self.dst
        for d in order:
            there = dst.at[rem(n.z + 8 - d, 8), n.y]
            if d:
                n.got(self.zc[d])
            piece = there if d else self.src
            self.ups[d] = n.send(piece, there, dy=1)
            self.downs[d] = n.send(piece, there, dy=3)

    def across(self, order):
        n, dst = self.n, self.dst
        last = []
        for d in order:
            zs = rem(n.z + 8 - d, 8)
            if d in UPWARD:
                n.got(self.ups[d])
                piece = dst.at[zs, rem(n.y + 3, 4)]
                last.append(n.send(piece, piece, dy=1))
            else:
                n.got(self.downs[d])
                piece = dst.at[zs, rem(n.y + 1, 4)]
                last.append(n.send(piece, piece, dy=3))
        for d in order:
            n.got(self.downs[d] if d in UPWARD else self.ups[d])
        return last


def high_low_pair(v, lane):
    high = v.astype(BF).astype(F32)
    return high + pltpu.roll(v - high, 1, 1)


def dispatch(
    Hd, MO, PG, TO, GA, DGO, DGF, DM, Gx, Hid, Hq,
    Hg, mx, Mx, Hx, S, A, Pd, B2, Q, Q2, ssem, rsem, lsem,
):
    n = Net(ssem, rsem, lsem)
    j = n.y * 2 + n.c
    n.enter(ZP + YC + XP)
    g = Gather(n, Hd, Hg)
    g.onward([0] + ZS)
    for copy in g.across([0] + ZS):
        n.got(copy)
    w = MO[...] + PG[0:512]
    mx[...] = (
        jnp.dot(Hg[...].reshape(512, 512), w, preferred_element_type=F32)
        .astype(BF)
        .reshape(4, 128, 128)
    )
    xs = [n.send(mx.at[rem(n.x + p["dx"], 4)], Mx.at[n.x], **p) for p in XP]
    Mx[n.x] = mx[n.x]
    own = pl.ds(pl.multiple_of(n.x * 128, 128), 128)
    token = TO[own, :].astype(F32) + PG[pl.ds(pl.multiple_of(512 + n.x * 128, 128), 128), :].astype(F32)
    for copy in xs:
        n.got(copy)
    mixer = jnp.sum(Mx[...].astype(F32), axis=0).astype(BF)
    hb = (token + mixer.astype(F32)).astype(BF)
    Hq[...] = hb
    Hx[n.x] = hb
    hs = [n.send(Hq, Hx.at[n.x], **p) for p in XP]
    S[...] = jnp.dot(DM[...], hb, preferred_element_type=F32).astype(BF).reshape(8, 8, 16, 128)
    zc = {d: n.send(S.at[rem(n.z + d, 8)], A.at[n.z], dz=d) for d in ZS}

    yc, local = {}, {}

    def around(d):
        zs = rem(n.z + 8 - d, 8)
        if d:
            n.got(zc[d])
        piece = A.at[zs] if d else S.at[n.z]
        yc[d] = []
        for p in YC:
            to = rem(n.y + p["dy"], 4) * 2 + core_of(n, p)
            yc[d].append(n.send(piece.at[to], Gx.at[n.x, zs, j], **p))
        local[d] = n.local(piece.at[j], Gx.at[n.x, zs, j])

    around(0)
    for copy in hs:
        n.got(copy)
    h = Hx[...].reshape(512, 128).astype(F32)
    gain, mix = GA[n.z, pl.ds(n.y, 1), :], GA[n.z, pl.ds(n.y + 4, 1), :]
    hg = h * gain
    lane = lax.broadcasted_iota(jnp.int32, (512, 128), 1)
    stats = jnp.where(
        lane == 0,
        jnp.sum(h * h, axis=1, keepdims=True),
        jnp.where(lane == 2, jnp.sum(hg * mix, axis=1, keepdims=True), 0.0),
    )
    first = n.c == 0
    w = jnp.concatenate(
        [jnp.where(first, DGO[...], DGF[...]), jnp.where(first, DGF[...], DGO[...])], axis=0
    )
    part = jnp.dot(hg.astype(BF), w, preferred_element_type=F32).astype(BF).reshape(8, 4, 16, 512)
    stat = high_low_pair(stats, lane).astype(BF).reshape(8, 4, 16, 128)
    for y in range(4):
        Pd[y, :, :, 0:512] = part[:, y]
        Pd[y, :, :, 512:640] = stat[:, y]
    ds = [n.send(Pd.at[rem(n.y + p["dy"], 4)], B2.at[n.y], **p) for p in YP]
    B2[n.y] = Pd[n.y]
    for d in ZS:
        around(d)
    ups, downs = {}, {}
    for d in [0] + ZS:
        for copy in yc[d]:
            n.got(copy)
        local[d].wait()
        piece = Gx.at[n.x, rem(n.z + 8 - d, 8)]
        ups[d] = n.send(piece, piece, dx=1)
        downs[d] = n.send(piece, piece, dx=3)
    for copy in ds:
        n.got(copy)
    total = jnp.sum(B2[...].astype(F32), axis=0).reshape(128, 640)
    ext = total[:, 512:640]
    lane = lax.broadcasted_iota(jnp.int32, (128, 128), 1)
    ext = jnp.where((lane == 0) | (lane == 2), ext + pltpu.roll(ext, 127, 1), 0.0)
    Q[:, :, 0:512] = total[:, 0:512].astype(BF).reshape(8, 16, 512)
    Q[:, :, 512:640] = high_low_pair(ext, lane).astype(BF).reshape(8, 16, 128)
    qs = [n.send(Q.at[rem(n.z + d, 8)], Q2.at[n.z], dz=d) for d in ZS]
    Q2[n.z] = Q[n.z]
    for d in [0] + ZS:
        if d in UPWARD:
            n.got(ups[d])
            piece = Gx.at[rem(n.x + 3, 4), rem(n.z + 8 - d, 8)]
            n.send(piece, piece, dx=1)
        else:
            n.got(downs[d])
            piece = Gx.at[rem(n.x + 1, 4), rem(n.z + 8 - d, 8)]
            n.send(piece, piece, dx=3)
    for copy in qs:
        n.got(copy)
    s = jnp.sum(Q2[...].astype(F32), axis=0)
    ext = s[:, 512:640]
    inv = lax.rsqrt((ext[:, 0:1] + ext[:, 1:2]) * (1.0 / D) + EPSILON)
    gate = inv * (ext[:, 2:3] + ext[:, 3:4])
    gp = s[:, 0:256] * inv
    up = s[:, 256:512] * inv
    Hid[...] = (gp / (1.0 + jnp.exp(-gp)) * up / (1.0 + jnp.exp(-gate))).astype(BF)
    n.finish()


def collect(
    O, Hd, DO, PG, DH, DL, Hq, Fo,
    Og, R, A, B, Hg, Dp, Dq, out, ssem, rsem, lsem,
):
    n = Net(ssem, rsem, lsem)
    j = n.y * 2 + n.c
    n.enter(ZP + YC + XP)
    far = [4, 3, 5, 2, 6, 1, 7, 0]
    g = Gather(n, Hd, Hg)
    xs, zc = {}, {}
    for d in far:
        zt = rem(n.z + d, 8)
        xs[d] = [n.send(O.at[rem(n.x + p["dx"], 4), zt], Og.at[n.x, zt], **p) for p in XP]

    def summed(d):
        zt = rem(n.z + d, 8)
        for copy in xs[d]:
            n.got(copy)
        acc = O[n.x, zt].astype(F32)
        for p in XP:
            acc = acc + Og[rem(n.x + p["dx"], 4), zt].astype(F32)
        R[zt] = acc.astype(BF)
        if d:
            zc[d] = n.send(R.at[zt], A.at[n.z], dz=d)

    def around(d):
        zs = rem(n.z + 8 - d, 8)
        if d:
            n.got(zc[d])
        piece = A.at[zs] if d else R.at[n.z]
        for p in YC:
            to = rem(n.y + p["dy"], 4) * 2 + core_of(n, p)
            n.send(piece.at[to], B.at[zs, j], **p)
        B[zs, j] = piece[j]

    summed(4)
    summed(3)
    summed(5)
    g.onward([0] + ZS)
    summed(2)
    around(4)
    summed(6)
    around(3)
    last = g.across([0] + ZS)
    summed(1)
    around(5)
    for copy in last:
        n.got(copy)
    w = DO[...] + PG[1024:1280]
    Dp[...] = (
        jnp.dot(Hg[...].reshape(512, 256), w, preferred_element_type=F32)
        .astype(BF)
        .reshape(4, 128, 128)
    )
    for p in XP:
        n.send(Dp.at[rem(n.x + p["dx"], 4)], Dq.at[n.x], **p)
    Dq[n.x] = Dp[n.x]
    summed(7)
    around(2)
    summed(0)
    around(0)
    for d in (6, 1, 7):
        around(d)
    n.flush()
    got = B[...].reshape(1024, 128)
    routed = jnp.dot(DH[...], got, preferred_element_type=F32)
    routed += jnp.dot(DL[...], got, preferred_element_type=F32)
    dense = jnp.sum(Dq[...].astype(F32), axis=0)
    out[...] = (Hq[...].astype(F32) + routed + dense).astype(BF)
    cs = [n.send(out, Fo.at[n.c, n.x], **p) for p in XP]
    n.send(out, Fo.at[n.c, n.x], dc=1)
    Fo[n.c, n.x] = out[...]
    for p, copy in zip(XP, cs):
        n.got(copy)
        piece = Fo.at[n.c, rem(n.x + 4 - p["dx"], 4)]
        n.send(piece, piece, dc=1)
    n.finish()


def plain(body, ins, outs, grid=None, in_specs=None, out_specs=None, scratch=(), sems=0):
    vmem = pl.BlockSpec(memory_space=pltpu.VMEM)
    kw = {}
    if grid is not None:
        kw = dict(grid=grid)
    return pl.pallas_call(
        body,
        out_shape=[jax.ShapeDtypeStruct(s, t) for s, t in outs],
        in_specs=in_specs or [vmem] * len(ins),
        out_specs=out_specs or [vmem] * len(outs),
        scratch_shapes=[pltpu.VMEM(s, t) for s, t in scratch]
        + ([pltpu.SemaphoreType.DMA((sems,))] if sems else []),
        compiler_params=pltpu.CompilerParams(vmem_limit_bytes=40 * 1024 * 1024),
        name=body.__name__,
        **kw,
    )(*ins)


def prep(
    vec, tokens, wq, wk, wv, wo, wi, wf, wm, wg, wu, wd, routes, weights,
    W, T, S, G, TO, PR, MO, DO, DG, DM, DH, DL,
    tk, gi, gf, sm, sd, rt, rw, sem,
):
    z, y, c, x = coords()
    copies = [
        (tokens, tk),
        (wi, gi),
        (wf, gf),
        (wq, W.at[:, pl.ds(128, 256)]),
        (wk, W.at[:, pl.ds(384, 256)]),
        (wv, W.at[:, pl.ds(640, 512)]),
        (wo, W.at[:, pl.ds(1152, 512)]),
        (wm, sm),
        (wg, DG.at[:, pl.ds(0, 256)]),
        (wu, DG.at[:, pl.ds(256, 256)]),
        (wd, sd),
    ]
    for b in range(8):
        block = (x * 2 + b // 4) * 8 + (b % 4) * 2 + c
        at = pl.ds(pl.multiple_of(block * 16, 16), 16)
        copies.append((routes.at[at], rt.at[pl.ds(b * 16, 16)]))
        copies.append((weights.at[at], rw.at[pl.ds(b * 16, 16)]))
    started = []
    for i, (src, dst) in enumerate(copies):
        copy = pltpu.make_async_copy(src, dst, sem.at[i])
        copy.start()
        started.append(copy)
    vt = jnp.concatenate([vec[...], jnp.zeros((112, 128), F32)], axis=0).T
    row = lax.broadcasted_iota(jnp.int32, (8, 128), 0)
    gain, mix = vec[1:2, :], vec[2:3, :]
    place = lambda v: jnp.where(c == 0, v, pltpu.roll(v, 64, 1))
    G[...] = jnp.where(row == y, place(gain), jnp.where(row == y + 4, place(mix), 0.0))
    for copy in started:
        copy.wait()

    def half(v):
        zero = jnp.zeros(v.shape, v.dtype)
        low = jnp.concatenate([v, zero], axis=1)
        high = jnp.concatenate([zero, v], axis=1)
        return jnp.where(c == 0, low, high)

    W[:, 0:128] = jnp.concatenate(
        [jnp.zeros((64, 8), BF), gi[...], gf[...], jnp.zeros((64, 112), BF)], axis=1
    )
    MO[...] = half(sm[...])
    DO[...] = half(sd[...])
    PR[0:512, :] = MO[...]
    PR[1024:1280, :] = DO[...]
    grid = tk[...].reshape(8, 4, 2, 16, 64)
    even = grid[:, :, 0].reshape(512, 64)
    odd = grid[:, :, 1].reshape(512, 64)
    TO[...] = half(jnp.where(c == 0, even, odd))
    PR[512:1024, :] = half(jnp.where(c == 0, odd, even))
    eight = tk[...].reshape(8, 8, 16, 64)
    for j in range(8):
        block = eight[:, j].reshape(128, 64).astype(F32)
        wide = jnp.concatenate([block, jnp.zeros((128, 64), F32)], axis=1).T[0:64]
        T[j] = (wide * vt[0:64, 0:1]).astype(BF)
        S[j] = jnp.where(row == 0, jnp.sum(wide * wide, axis=0, keepdims=True), 0.0)

    def turned(v):
        return jnp.concatenate([v.astype(F32), jnp.zeros((128, 124), F32)], axis=1).T

    named, given = turned(rt[...]), turned(rw[...])
    expert = lax.broadcasted_iota(jnp.int32, (64, 128), 0).astype(F32)
    picked = jnp.zeros((64, 128), F32)
    weight = jnp.zeros((64, 128), F32)
    for i in range(4):
        hit = named[i : i + 1, :] == expert
        picked = picked + jnp.where(hit, 1.0, 0.0)
        weight = weight + jnp.where(hit, given[i : i + 1, :], 0.0)
    r = lax.broadcasted_iota(jnp.int32, (128, 128), 0)
    t = lax.broadcasted_iota(jnp.int32, (128, 128), 1)
    earlier = jnp.where((lax.shift_right_logical(r, 4) == lax.shift_right_logical(t, 4)) & (r < t), 1.0, 0.0)
    rank = jnp.dot(picked.astype(BF), earlier.astype(BF), preferred_element_type=F32)
    slot = lax.broadcasted_iota(jnp.int32, (1, 16, 128), 1)
    to = lax.broadcasted_iota(jnp.int32, (1, 16, 128), 2)
    fits = jnp.where(lax.shift_right_logical(slot, 1) == lax.shift_right_logical(to, 4), 1.0, 0.0)
    turn = (slot & 1).astype(F32)
    shape = (64, 16, 128)
    taken = jnp.where(
        jnp.broadcast_to(rank[:, None, :], shape) == jnp.broadcast_to(turn, shape),
        jnp.broadcast_to(picked[:, None, :], shape) * jnp.broadcast_to(fits, shape),
        0.0,
    )
    DM[...] = taken.reshape(1024, 128).astype(BF)
    weighted = (taken * jnp.broadcast_to(weight[:, None, :], shape)).reshape(1024, 128).T
    high = weighted.astype(BF)
    DH[...] = high
    DL[...] = (weighted - high.astype(F32)).astype(BF)


def log_sigmoid(v):
    return jnp.minimum(v, 0.0) - jnp.log1p(jnp.exp(-jnp.abs(v)))


def cell(Mg, GB, SM, HG, SN, ST, NM, NN, NX, HO, qt, kt, vv, cc, oo, num, dn):
    step = pl.program_id(0)

    @pl.when(step == 0)
    def _():
        acc = jnp.sum(Mg[...].astype(F32), axis=0)
        ext = acc[:, 0:128] + pltpu.roll(acc[:, 0:128], 64, 1)
        inv = lax.rsqrt(ext[:, 0:1] * (1.0 / D) + EPSILON)
        proj = (acc[:, 128:] * inv).astype(BF).astype(F32)
        pre = ext * inv
        in_log = SOFT_CAP * jnp.tanh((pre + GB[3:4, :]) / SOFT_CAP)
        forget = pltpu.roll(pre, 124, 1)
        forget_log = log_sigmoid(SOFT_CAP * jnp.tanh((forget + GB[4:5, :]) / SOFT_CAP))
        smax = jnp.concatenate(
            [jnp.zeros((16, 8), F32), SM[...], jnp.zeros((16, 116), F32)], axis=1
        )
        new_max = jnp.maximum(forget_log + smax, in_log)
        carried = jnp.exp(forget_log + smax - new_max)
        fresh = jnp.exp(in_log - new_max)
        floor = jnp.exp(-new_max)
        NX[...] = new_max[:, 8:12]
        cc[...] = carried
        q = proj[:, 0:256] * 0.125
        k = proj[:, 256:512]
        vv[...] = proj[:, 512:1024]
        oo[...] = proj[:, 1024:1536]
        fk = []
        for h in range(4):
            lane = slice(8 + h, 9 + h)
            kh = k[:, h * 64 : (h + 1) * 64] * fresh[:, lane]
            qh = q[:, h * 64 : (h + 1) * 64]
            nn = carried[:, lane] * SN[:, h, :] + kh
            NN[:, h, :] = nn
            den = jnp.sum(nn * qh, axis=1, keepdims=True)
            dn[:, h * 128 : (h + 1) * 128] = jnp.broadcast_to(
                jnp.maximum(jnp.abs(den), floor[:, lane]), (16, 128)
            )
            fk.append(kh)
        fk = jnp.concatenate(fk, axis=1)
        zeros = jnp.zeros((112, 256), F32)
        qt[...] = jnp.concatenate([q, zeros], axis=0).T
        kt[...] = jnp.concatenate([fk, zeros], axis=0).T

    shift = rem(128 - step * 4, 128)
    qr = pltpu.roll(qt[...], shift, 1)
    kr = pltpu.roll(kt[...], shift, 1)
    for r in range(4):
        row = step * 4 + r
        crow = cc[pl.ds(row, 1), :]
        vrow = vv[pl.ds(row, 1), :]
        for h in range(4):
            qc = jnp.broadcast_to(qr[h * 64 : (h + 1) * 64, r : r + 1], (64, 128))
            kc = jnp.broadcast_to(kr[h * 64 : (h + 1) * 64, r : r + 1], (64, 128))
            new = crow[:, 8 + h : 9 + h] * ST[r, h] + kc * vrow[:, h * 128 : (h + 1) * 128]
            NM[r, h] = new
            num[row, :, h * 128 : (h + 1) * 128] = jnp.sum(new * qc, axis=0, keepdims=True)

    @pl.when(step == 3)
    def _():
        read = jnp.concatenate([num[i] for i in range(16)], axis=0) / dn[...]
        parts = []
        for h in range(4):
            rh = read[:, h * 128 : (h + 1) * 128]
            parts.append(
                rh * lax.rsqrt(jnp.mean(rh * rh, axis=1, keepdims=True) + EPSILON)
            )
        gain = jnp.concatenate([HG[8 + h : 9 + h, :] for h in range(4)], axis=1)
        scaled = jnp.concatenate(parts, axis=1) * gain
        HO[...] = (scaled / (1.0 + jnp.exp(-oo[...]))).astype(BF)


def run_cell(mg, vec, sm, sn, st):
    full = lambda s: pl.BlockSpec(s, lambda i: (0,) * len(s))
    state = pl.BlockSpec((4, 4, 64, 128), lambda i: (i, 0, 0, 0))
    return plain(
        cell,
        (mg, vec, sm, vec, sn, st),
        [((16, 4, 64, 128), F32), ((16, 4, 64), F32), ((16, 4), F32), ((16, 512), BF)],
        grid=(4,),
        in_specs=[
            full((8, 16, 1664)),
            full((16, 128)),
            full((16, 4)),
            full((16, 128)),
            full((16, 4, 64)),
            state,
        ],
        out_specs=[state, full((16, 4, 64)), full((16, 4)), full((16, 512))],
        scratch=[
            ((256, 128), F32),
            ((256, 128), F32),
            ((16, 512), F32),
            ((16, 128), F32),
            ((16, 512), F32),
            ((16, 1, 512), F32),
            ((16, 512), F32),
        ],
    )


def ffn(Gx, GA, WG, WU, WD, O, ga, ua, sq):
    step = pl.program_id(0)

    @pl.when(step == 0)
    def _():
        ga[...] = jnp.zeros_like(ga)
        ua[...] = jnp.zeros_like(ua)
        sq[...] = jnp.zeros_like(sq)

    parts = []
    s2 = sq[...]
    for y in range(4):
        block = Gx[:, 0, 2 * y : 2 * y + 2].reshape(128, 128).astype(F32)
        s2 = s2 + block * block
        gain = GA[0, y : y + 1, :]
        parts.append((block * gain).astype(BF))
    sq[...] = s2
    rows = jnp.concatenate(parts, axis=1)
    ga[...] += jnp.dot(rows, WG[0], preferred_element_type=F32)
    ua[...] += jnp.dot(rows, WU[0], preferred_element_type=F32)

    @pl.when(step == 7)
    def _():
        inv = lax.rsqrt(jnp.sum(sq[...], axis=1, keepdims=True) * (1.0 / D) + EPSILON)
        g = ga[...] * inv
        u = ua[...] * inv
        hid = (g / (1.0 + jnp.exp(-g)) * u).astype(BF)

        def out(zy, carry):
            at = pl.multiple_of(zy * 512, 512)
            res = jnp.dot(hid, WD[0, :, pl.ds(at, 512)], preferred_element_type=F32).astype(BF)
            for y in range(4):
                for c in range(2):
                    for x in range(4):
                        O[x, zy, 2 * y + c] = res[
                            (x * 2 + c) * 16 : (x * 2 + c + 1) * 16, y * 128 : (y + 1) * 128
                        ]
            return carry

        lax.fori_loop(0, 8, out, 0)


def run_ffn(gx, gall, wg, wu, wd):
    full = lambda s: pl.BlockSpec(s, lambda i: (0,) * len(s))
    return plain(
        ffn,
        (gx, gall, wg, wu, wd),
        [((4, 8, 8, 16, 128), BF)],
        grid=(8,),
        in_specs=[
            pl.BlockSpec((4, 1, 8, 16, 128), lambda i: (0, i, 0, 0, 0)),
            pl.BlockSpec((1, 8, 128), lambda i: (i, 0, 0)),
            pl.BlockSpec((1, 512, 256), lambda i: (0, i, 0)),
            pl.BlockSpec((1, 512, 256), lambda i: (0, i, 0)),
            full((1, 256, 4096)),
        ],
        out_specs=[full((4, 8, 8, 16, 128))],
        scratch=[((128, 256), F32), ((128, 256), F32), ((128, 128), F32)],
    )[0]


def on_device(
    tokens,
    mix_gain,
    w_query,
    w_key,
    w_value,
    w_outgate,
    w_igate,
    w_fgate,
    igate_bias,
    fgate_bias,
    head_gain,
    w_mixout,
    state_matrix,
    state_norm,
    state_max,
    ffn_gain,
    dense_mix,
    w_dense_gate,
    w_dense_up,
    w_dense_down,
    routes,
    route_weights,
    w_exp_gate,
    w_exp_up,
    w_exp_down,
):
    c = rem(lax.axis_index("ep"), 2)

    def line(v, at, lane=0):
        v = v.astype(F32).reshape(-1, min(v.shape[0], 128))
        rows, lanes = v.shape
        return jnp.pad(v, ((at, 16 - at - rows), (lane, 128 - lane - lanes)))

    vec = line(mix_gain, 0) + line(ffn_gain, 1) + line(dense_mix, 2)
    vec = vec + line(igate_bias, 3, 8) + line(fgate_bias, 4, 8) + line(head_gain, 8)
    vmem, hbm = pl.BlockSpec(memory_space=pltpu.VMEM), pl.BlockSpec(memory_space=pl.ANY)
    W, T, S, G, TO, PR, MO, DO, DG, DM, DH, DL = plain(
        prep,
        (
            vec, tokens, w_query, w_key, w_value, w_outgate, w_igate, w_fgate, w_mixout,
            w_dense_gate, w_dense_up, w_dense_down, routes, route_weights,
        ),
        [
            ((64, 1664), BF),
            ((8, 64, 128), BF),
            ((8, 8, 128), F32),
            ((8, 128), F32),
            ((512, 128), BF),
            ((1280, 128), BF),
            ((512, 128), BF),
            ((256, 128), BF),
            ((64, 512), BF),
            ((1024, 128), BF),
            ((128, 1024), BF),
            ((128, 1024), BF),
        ],
        in_specs=[vmem] + [hbm] * 13,
        scratch=[
            ((1024, 64), BF),
            ((64, 4), BF),
            ((64, 4), BF),
            ((512, 64), BF),
            ((256, 64), BF),
            ((128, 4), jnp.int32),
            ((128, 4), F32),
        ],
        sems=27,
    )
    Mg, GA, Pg, Dg = exchange(
        project,
        (W, T, S, G, PR, DG),
        [((8, 16, 1664), BF), ((8, 8, 128), F32), ((1280, 128), BF), ((64, 512), BF)],
        [
            ((8, 64, 1664), BF),
            ((8, 64, 128), BF),
            ((8, 8, 128), F32),
            ((8, 8, 128), F32),
            ((8, 16, 1664), BF),
            ((8, 128), F32),
        ],
        72,
        0,
    )
    new_matrix, new_norm, new_max, heads = run_cell(Mg, vec, state_max, state_norm, state_matrix)
    Gx, hidden, hq = exchange(
        dispatch,
        (heads, MO, Pg, TO, GA, DG, Dg, DM),
        [((4, 8, 8, 16, 128), BF), ((16, 256), BF), ((128, 128), BF)],
        [
            ((8, 4, 16, 512), BF),
            ((4, 128, 128), BF),
            ((4, 128, 128), BF),
            ((4, 128, 128), BF),
            ((8, 8, 16, 128), BF),
            ((8, 8, 16, 128), BF),
            ((4, 8, 16, 640), BF),
            ((4, 8, 16, 640), BF),
            ((8, 16, 640), BF),
            ((8, 16, 640), BF),
        ],
        134,
        1,
    )
    O = run_ffn(Gx, GA, w_exp_gate, w_exp_up, w_exp_down)
    (Fo,) = exchange(
        collect,
        (O, hidden, DO, Pg, DH, DL, hq),
        [((2, 4, 128, 128), BF)],
        [
            ((4, 8, 8, 16, 128), BF),
            ((8, 8, 16, 128), BF),
            ((8, 8, 16, 128), BF),
            ((8, 8, 16, 128), BF),
            ((8, 4, 16, 256), BF),
            ((4, 128, 128), BF),
            ((4, 128, 128), BF),
            ((128, 128), BF),
        ],
        128,
        2,
    )
    both = Fo.reshape(2, 32, 16, 128)
    mine = jnp.where(c == 0, both[..., :64], both[..., 64:])
    layer_out = mine.transpose(1, 0, 2, 3).reshape(1024, 64)
    return (layer_out, new_matrix, new_norm, new_max)


def solution(mesh):
    return jax.shard_map(
        on_device,
        mesh=mesh,
        in_specs=(
            P(None, "ep"),
            P("ep"),
            P("ep", "tp"),
            P("ep", "tp"),
            P("ep", "tp"),
            P("ep", "tp"),
            P("ep", "tp"),
            P("ep", "tp"),
            P("tp"),
            P("tp"),
            P("tp"),
            P("tp", "ep"),
            P("ep", "tp", None, None),
            P("ep", "tp", None),
            P("ep", "tp"),
            P("ep"),
            P("ep"),
            P("ep", "tp"),
            P("ep", "tp"),
            P("tp", "ep"),
            P(),
            P(),
            P("ep", None, "tp"),
            P("ep", None, "tp"),
            P("ep", "tp", None),
        ),
        out_specs=(P(None, "ep"), P("ep", "tp", None, None), P("ep", "tp", None), P("ep", "tp")),
        check_vma=False,
    )
```

```python
import jax
import jax.numpy as jnp
from jax import lax
from jax.experimental import pallas as pl
from jax.experimental.pallas import tpu as pltpu
from jax.sharding import PartitionSpec as P

D = 4096
EPSILON = 1e-06
SOFT_CAP = 15.0
BF, F32 = jnp.bfloat16, jnp.float32
MESH = pl.DeviceIdType.MESH


def rem(a, n):
    return lax.rem(a, jnp.int32(n))


def div(a, n):
    return lax.div(a, jnp.int32(n))


def coords():
    e, x = lax.axis_index("ep"), lax.axis_index("tp")
    return div(e, 8), div(rem(e, 8), 2), rem(e, 2), x


class Net:
    def __init__(self, ssem, rsem, lsem):
        self.ssem, self.rsem, self.lsem = ssem, rsem, lsem
        self.at, self.lat = 0, 0
        self.open = []
        self.z, self.y, self.c, self.x = coords()

    def dev(self, dz=0, dy=0, dc=0, dx=0):
        z = rem(self.z + dz, 8) if dz else self.z
        y = rem(self.y + dy, 4) if dy else self.y
        c = 1 - self.c if dc else self.c
        x = rem(self.x + dx, 4) if dx else self.x
        return {"ep": z * 8 + y * 2 + c, "tp": x}

    def enter(self, peers):
        barrier = pltpu.get_barrier_semaphore()
        for p in peers:
            pl.semaphore_signal(barrier, inc=1, device_id=self.dev(**p), device_id_type=MESH)
        pl.semaphore_wait(barrier, len(peers))

    def send(self, src, dst, **peer):
        copy = pltpu.make_async_remote_copy(
            src_ref=src,
            dst_ref=dst,
            send_sem=self.ssem.at[self.at],
            recv_sem=self.rsem.at[self.at],
            device_id=self.dev(**peer),
            device_id_type=MESH,
        )
        self.at += 1
        copy.start()
        self.open.append(copy)
        return copy

    def local(self, src, dst):
        copy = pltpu.make_async_copy(src, dst, self.lsem.at[self.lat])
        self.lat += 1
        copy.start()
        return copy

    def got(self, copy):
        copy.wait_recv()
        copy.got = True

    def flush(self):
        for copy in self.open:
            if not getattr(copy, "got", False):
                self.got(copy)

    def finish(self):
        self.flush()
        for copy in self.open:
            copy.wait_send()


def exchange(body, ins, outs, scratch, copies, cid, hbm=(), limit=16 * 1024):
    vmem, far = pl.BlockSpec(memory_space=pltpu.VMEM), pl.BlockSpec(memory_space=pltpu.HBM)
    return pl.pallas_call(
        body,
        out_shape=[jax.ShapeDtypeStruct(s, t) for s, t in outs],
        in_specs=[far if i in hbm else vmem for i in range(len(ins))],
        out_specs=[vmem] * len(outs),
        scratch_shapes=[pltpu.VMEM(s, t) for s, t in scratch]
        + [
            pltpu.SemaphoreType.DMA((copies,)),
            pltpu.SemaphoreType.DMA((copies,)),
            pltpu.SemaphoreType.DMA((16,)),
        ],
        compiler_params=pltpu.CompilerParams(
            collective_id=cid, has_side_effects=True, vmem_limit_bytes=limit * 1024
        ),
        name=body.__name__,
    )(*ins)


YC = [dict(dy=dy, dc=dc) for dy in range(4) for dc in range(2) if dy or dc]
ZS = [1, 7, 2, 6, 3, 5, 4]
ZP = [dict(dz=d) for d in ZS]
YP = [dict(dy=d) for d in (1, 3, 2)]
XP = [dict(dx=d) for d in (1, 3, 2)]


UPWARD = (0, 1, 2, 4)


def core_of(n, p):
    return 1 - n.c if p["dc"] else n.c


def project(W, T, S, G, PR, DG, MO, DO, Mg, GA, Pg, Dg, Mf, Df, Wg, Tg, Sg, Gg, M, Gz, ssem, rsem, lsem):
    n = Net(ssem, rsem, lsem)
    j = n.y * 2 + n.c
    n.enter(YC + ZP)
    small = []
    for p in YC:
        to = rem(n.y + p["dy"], 4) * 2 + core_of(n, p)
        small.append(n.send(T.at[to], Tg.at[j], **p))
        small.append(n.send(S.at[to], Sg.at[j], **p))
    spans = [pl.ds(0, 640), pl.ds(640, 512), pl.ds(1152, 512)]
    ys, cs = [], []
    for ch in spans:
        cs.append([n.send(W.at[:, ch], Wg.at[j, :, ch], dc=1)])
        ys.append([n.send(W.at[:, ch], Wg.at[j, :, ch], **p) for p in YP])
    gs = [n.send(G, Gg.at[j], **p) for p in YC]
    for mine, there in ((PR, Pg), (DG, Dg), (MO, Mf), (DO, Df)):
        n.send(mine, there, dc=1)
    Wg[j] = W[...]
    Tg[j] = T[j]
    Sg[j] = S[j]
    Gg[j] = G[...]
    a = None
    for i, ch in enumerate(spans):
        for p, copy in zip(YP, ys[i]):
            n.got(copy)
            piece = Wg.at[rem(n.y + 4 - p["dy"], 4) * 2 + n.c, :, ch]
            cs[i].append(n.send(piece, piece, dc=1))
        if i == 0:
            for copy in small:
                n.got(copy)
            a = Tg[...].reshape(512, 128).T
        for copy in cs[i]:
            n.got(copy)
        w = Wg[:, :, ch].reshape(512, ch.size)
        res = jnp.dot(a, w, preferred_element_type=F32)
        if i == 0:
            ss = jnp.sum(Sg[...], axis=0)
            ext = res[:, 0:128] + jnp.concatenate([ss, jnp.zeros((120, 128), F32)], axis=0).T
            high = ext.astype(BF).astype(F32)
            ext = high + pltpu.roll(ext - high, 64, 1)
            M[:, :, 0:128] = ext.astype(BF).reshape(8, 16, 128)
            M[:, :, 128:640] = res[:, 128:].astype(BF).reshape(8, 16, 512)
        else:
            M[:, :, ch] = res.astype(BF).reshape(8, 16, 512)
        for d in ZS:
            n.send(M.at[rem(n.z + d, 8), :, ch], Mg.at[n.z, :, ch], dz=d)
    for copy in gs:
        n.got(copy)
    Gz[...] = jnp.sum(Gg[...], axis=0)
    for d in ZS:
        n.send(Gz, GA.at[n.z], dz=d)
    GA[n.z] = Gz[...]
    Mg[n.z] = M[n.z]
    n.finish()


class Gather:
    def __init__(self, n, src, dst):
        self.n, self.src, self.dst = n, src, dst
        self.zc = {d: n.send(src, dst.at[n.z, n.y], dz=d) for d in ZS}
        dst[n.z, n.y] = src[...]
        self.ups, self.downs = {}, {}

    def onward(self, order):
        n, dst = self.n, self.dst
        for d in order:
            there = dst.at[rem(n.z + 8 - d, 8), n.y]
            if d:
                n.got(self.zc[d])
            piece = there if d else self.src
            self.ups[d] = n.send(piece, there, dy=1)
            self.downs[d] = n.send(piece, there, dy=3)

    def across(self, order):
        n, dst = self.n, self.dst
        last = []
        for d in order:
            zs = rem(n.z + 8 - d, 8)
            if d in UPWARD:
                n.got(self.ups[d])
                piece = dst.at[zs, rem(n.y + 3, 4)]
                last.append(n.send(piece, piece, dy=1))
            else:
                n.got(self.downs[d])
                piece = dst.at[zs, rem(n.y + 1, 4)]
                last.append(n.send(piece, piece, dy=3))
        for d in order:
            n.got(self.downs[d] if d in UPWARD else self.ups[d])
        return last


def high_low_pair(v, lane):
    high = v.astype(BF).astype(F32)
    return high + pltpu.roll(v - high, 1, 1)


NT = (((1,), (1,)), ((), ()))


def branches(
    Hd, MO, MF, PG, TO, GA, DGO, DGF, DM, DO, DF, DH, DL, WGh, WUh, WDh,
    Fo,
    Hg, mx, Mx, Hq, Hx, S, A, Pd, B2, Q, Q2, Gx, Hid, WG, WU, WD, ga, ua, sq,
    O, Og, R, A2, B, Hg2, Dp, Dq, out, ssem, rsem, lsem,
):
    n = Net(ssem, rsem, lsem)
    j = n.y * 2 + n.c
    weights = [n.local(WGh.at[0], WG), n.local(WUh.at[0], WU), n.local(WDh.at[0], WD)]
    n.enter(ZP + YC + XP)
    g = Gather(n, Hd, Hg)
    g.onward([0] + ZS)
    for copy in g.across([0] + ZS):
        n.got(copy)
    first = n.c == 0

    def both(own, other):
        own, other = own[...], other[...]
        return jnp.concatenate(
            [jnp.where(first, own, other), jnp.where(first, other, own)], axis=0
        )

    mx[...] = (
        lax.dot_general(
            Hg[...].reshape(512, 512), both(MO, MF), NT, preferred_element_type=F32
        )
        .astype(BF)
        .reshape(4, 128, 128)
    )
    xs = [n.send(mx.at[rem(n.x + p["dx"], 4)], Mx.at[n.x], **p) for p in XP]
    Mx[n.x] = mx[n.x]
    own = pl.ds(pl.multiple_of(n.x * 128, 128), 128)
    token = TO[own, :].astype(F32) + PG[own, :].astype(F32)
    for copy in xs:
        n.got(copy)
    mixer = jnp.sum(Mx[...].astype(F32), axis=0).astype(BF)
    hb = (token + mixer.astype(F32)).astype(BF)
    Hq[...] = hb
    Hx[n.x] = hb
    hs = [n.send(Hq, Hx.at[n.x], **p) for p in XP]
    S[...] = jnp.dot(DM[...], hb, preferred_element_type=F32).astype(BF).reshape(8, 8, 16, 128)
    zc = {d: n.send(S.at[rem(n.z + d, 8)], A.at[n.z], dz=d) for d in ZS}
    yc, local = {}, {}

    def around(d):
        zs = rem(n.z + 8 - d, 8)
        if d:
            n.got(zc[d])
        piece = A.at[zs] if d else S.at[n.z]
        yc[d] = []
        for p in YC:
            to = rem(n.y + p["dy"], 4) * 2 + core_of(n, p)
            yc[d].append(n.send(piece.at[to], Gx.at[n.x, zs, j], **p))
        local[d] = n.local(piece.at[j], Gx.at[n.x, zs, j])

    around(0)
    for copy in hs:
        n.got(copy)
    h = Hx[...].reshape(512, 128).astype(F32)
    gain, mix = GA[n.z, pl.ds(n.y, 1), :], GA[n.z, pl.ds(n.y + 4, 1), :]
    hg = h * gain
    lane = lax.broadcasted_iota(jnp.int32, (512, 128), 1)
    stats = jnp.where(
        lane == 0,
        jnp.sum(h * h, axis=1, keepdims=True),
        jnp.where(lane == 2, jnp.sum(hg * mix, axis=1, keepdims=True), 0.0),
    )
    part = (
        jnp.dot(hg.astype(BF), both(DGO, DGF), preferred_element_type=F32)
        .astype(BF)
        .reshape(8, 4, 16, 512)
    )
    stat = high_low_pair(stats, lane).astype(BF).reshape(8, 4, 16, 128)
    for y in range(4):
        Pd[y, :, :, 0:512] = part[:, y]
        Pd[y, :, :, 512:640] = stat[:, y]
    ds = [n.send(Pd.at[rem(n.y + p["dy"], 4)], B2.at[n.y], **p) for p in YP]
    B2[n.y] = Pd[n.y]
    for d in ZS:
        around(d)
    ups, downs, fars = {}, {}, {}
    ga[...] = jnp.zeros_like(ga)
    ua[...] = jnp.zeros_like(ua)
    sq[...] = jnp.zeros_like(sq)

    def sideways(d):
        for copy in yc[d]:
            n.got(copy)
        local[d].wait()
        piece = Gx.at[n.x, rem(n.z + 8 - d, 8)]
        ups[d] = n.send(piece, piece, dx=1)
        downs[d] = n.send(piece, piece, dx=3)

    def onward(d):
        zs = rem(n.z + 8 - d, 8)
        if d in UPWARD:
            n.got(ups[d])
            piece = Gx.at[rem(n.x + 3, 4), zs]
            fars[d] = n.send(piece, piece, dx=1)
        else:
            n.got(downs[d])
            piece = Gx.at[rem(n.x + 1, 4), zs]
            fars[d] = n.send(piece, piece, dx=3)

    def expert(d):
        zs = rem(n.z + 8 - d, 8)
        n.got(downs[d] if d in UPWARD else ups[d])
        n.got(fars[d])
        parts = []
        s2 = sq[...]
        for y in range(4):
            block = Gx[:, zs, 2 * y : 2 * y + 2].reshape(128, 128).astype(F32)
            s2 = s2 + block * block
            parts.append((block * GA[zs, y : y + 1, :]).astype(BF))
        sq[...] = s2
        rows = jnp.concatenate(parts, axis=1)
        at = pl.ds(pl.multiple_of(zs * 512, 512), 512)
        ga[...] += jnp.dot(rows, WG[at, :], preferred_element_type=F32)
        ua[...] += jnp.dot(rows, WU[at, :], preferred_element_type=F32)

    def dense_down():
        for copy in ds:
            n.got(copy)
        total = jnp.sum(B2[...].astype(F32), axis=0).reshape(128, 640)
        ext = total[:, 512:640]
        lane = lax.broadcasted_iota(jnp.int32, (128, 128), 1)
        ext = jnp.where((lane == 0) | (lane == 2), ext + pltpu.roll(ext, 127, 1), 0.0)
        Q[:, :, 0:512] = total[:, 0:512].astype(BF).reshape(8, 16, 512)
        Q[:, :, 512:640] = high_low_pair(ext, lane).astype(BF).reshape(8, 16, 128)
        Q2[n.z] = Q[n.z]
        return [n.send(Q.at[rem(n.z + d, 8)], Q2.at[n.z], dz=d) for d in ZS]

    def dense_hidden(qs):
        for copy in qs:
            n.got(copy)
        s = jnp.sum(Q2[...].astype(F32), axis=0)
        ext = s[:, 512:640]
        inv = lax.rsqrt((ext[:, 0:1] + ext[:, 1:2]) * (1.0 / D) + EPSILON)
        gate = inv * (ext[:, 2:3] + ext[:, 3:4])
        gp = s[:, 0:256] * inv
        up = s[:, 256:512] * inv
        Hid[...] = (gp / (1.0 + jnp.exp(-gp)) * up / (1.0 + jnp.exp(-gate))).astype(BF)

    order = [0] + ZS
    for i in range(12):
        if i < 8:
            sideways(order[i])
        if i == 6:
            qs = dense_down()
        if 0 <= i - 2 < 8:
            onward(order[i - 2])
        if 0 <= i - 4 < 8:
            if i == 4:
                weights[0].wait()
                weights[1].wait()
            expert(order[i - 4])

    inv = lax.rsqrt(jnp.sum(sq[...], axis=1, keepdims=True) * (1.0 / D) + EPSILON)
    gp = ga[...] * inv
    hid = (gp / (1.0 + jnp.exp(-gp)) * (ua[...] * inv)).astype(BF)
    weights[2].wait()
    far = [4, 3, 5, 2, 6, 1, 7, 0]
    xo, zo = {}, {}
    for d in far:
        zt = rem(n.z + d, 8)
        at = pl.ds(pl.multiple_of(zt * 512, 512), 512)
        res = jnp.dot(hid, WD[:, at], preferred_element_type=F32).astype(BF)
        for y in range(4):
            for c in range(2):
                for x in range(4):
                    O[x, zt, 2 * y + c] = res[
                        (x * 2 + c) * 16 : (x * 2 + c + 1) * 16, y * 128 : (y + 1) * 128
                    ]
        xo[d] = [n.send(O.at[rem(n.x + p["dx"], 4), zt], Og.at[n.x, zt], **p) for p in XP]
        if d == 4:
            dense_hidden(qs)
            g = Gather(n, Hid, Hg2)

    def summed(d):
        zt = rem(n.z + d, 8)
        for copy in xo[d]:
            n.got(copy)
        acc = O[n.x, zt].astype(F32)
        for p in XP:
            acc = acc + Og[rem(n.x + p["dx"], 4), zt].astype(F32)
        R[zt] = acc.astype(BF)
        if d:
            zo[d] = n.send(R.at[zt], A2.at[n.z], dz=d)

    def back(d):
        zs = rem(n.z + 8 - d, 8)
        if d:
            n.got(zo[d])
        piece = A2.at[zs] if d else R.at[n.z]
        for p in YC:
            to = rem(n.y + p["dy"], 4) * 2 + core_of(n, p)
            n.send(piece.at[to], B.at[zs, j], **p)
        B[zs, j] = piece[j]

    summed(4)
    summed(3)
    summed(5)
    g.onward([0] + ZS)
    summed(2)
    back(4)
    summed(6)
    back(3)
    last = g.across([0] + ZS)
    summed(1)
    back(5)
    for copy in last:
        n.got(copy)
    Dp[...] = (
        lax.dot_general(
            Hg2[...].reshape(512, 256), both(DO, DF), NT, preferred_element_type=F32
        )
        .astype(BF)
        .reshape(4, 128, 128)
    )
    for p in XP:
        n.send(Dp.at[rem(n.x + p["dx"], 4)], Dq.at[n.x], **p)
    Dq[n.x] = Dp[n.x]
    summed(7)
    back(2)
    summed(0)
    back(0)
    for d in (6, 1, 7):
        back(d)
    n.flush()
    got = B[...].reshape(1024, 128)
    routed = jnp.dot(DH[...], got, preferred_element_type=F32)
    routed += jnp.dot(DL[...], got, preferred_element_type=F32)
    dense = jnp.sum(Dq[...].astype(F32), axis=0)
    out[...] = (Hq[...].astype(F32) + routed + dense).astype(BF)
    cs = [n.send(out, Fo.at[n.c, n.x], **p) for p in XP]
    n.send(out, Fo.at[n.c, n.x], dc=1)
    Fo[n.c, n.x] = out[...]
    for p, copy in zip(XP, cs):
        n.got(copy)
        piece = Fo.at[n.c, rem(n.x + 4 - p["dx"], 4)]
        n.send(piece, piece, dc=1)
    n.finish()


def plain(body, ins, outs, grid=None, in_specs=None, out_specs=None, scratch=(), sems=0, limit=16 * 1024):
    vmem = pl.BlockSpec(memory_space=pltpu.VMEM)
    kw = {}
    if grid is not None:
        kw = dict(grid=grid)
    return pl.pallas_call(
        body,
        out_shape=[jax.ShapeDtypeStruct(s, t) for s, t in outs],
        in_specs=in_specs or [vmem] * len(ins),
        out_specs=out_specs or [vmem] * len(outs),
        scratch_shapes=[pltpu.VMEM(s, t) for s, t in scratch]
        + ([pltpu.SemaphoreType.DMA((sems,))] if sems else []),
        compiler_params=pltpu.CompilerParams(vmem_limit_bytes=limit * 1024),
        name=body.__name__,
        **kw,
    )(*ins)


def prep(
    vec, big, small, table,
    W, T, S, G, TO, PR, MO, DO, DG, DM, DH, DL,
    tk,
):
    z, y, c, x = coords()
    W[:, 128:1664] = big[:, 0:1536]
    DG[...] = big[:, 1536:2048]
    MO[...] = big[:, 2048:2560]
    DO[...] = big[:, 2560:2816]
    vt = jnp.concatenate([vec[...], jnp.zeros((112, 128), F32)], axis=0).T
    row = lax.broadcasted_iota(jnp.int32, (8, 128), 0)
    gain, mix = vec[1:2, :], vec[2:3, :]

    def half(v):
        return jnp.where(c == 0, v, pltpu.roll(v, 64, 1))

    G[...] = jnp.where(row == y, half(gain), jnp.where(row == y + 4, half(mix), 0.0))
    gates = jnp.concatenate(
        [jnp.zeros((8, 64), F32), small[...].astype(F32), jnp.zeros((112, 64), F32)], axis=0
    )
    gates = jnp.concatenate([gates, jnp.zeros((128, 64), F32)], axis=1).T
    W[:, 0:128] = gates[0:64].astype(BF)
    for k in range(8):
        block = big[:, 2816 + k * 128 : 2944 + k * 128].astype(F32)
        tk[k * 128 : (k + 1) * 128, :] = jnp.concatenate(
            [block, jnp.zeros((64, 128), F32)], axis=0
        ).T
    grid = tk[...].reshape(8, 4, 2, 16, 128)
    even = grid[:, :, 0].reshape(512, 128)
    odd = grid[:, :, 1].reshape(512, 128)
    TO[...] = half(jnp.where(c == 0, even, odd)).astype(BF)
    PR[...] = half(jnp.where(c == 0, odd, even)).astype(BF)
    eight = tk[...].reshape(8, 8, 16, 128)
    for j in range(8):
        wide = eight[:, j].reshape(128, 128).T[0:64]
        T[j] = (wide * vt[0:64, 0:1]).astype(BF)
        S[j] = jnp.where(row == 0, jnp.sum(wide * wide, axis=0, keepdims=True), 0.0)

    mine = table[:, pl.ds(pl.multiple_of(x * 256, 256), 256)]
    mine = jnp.concatenate([mine, jnp.zeros((120, 256), F32)], axis=0)
    mine = jnp.concatenate([mine[:, 0:128].T, mine[:, 128:256].T], axis=0).reshape(8, 2, 16, 128)
    mine = jnp.where(c == 0, mine[:, 0].reshape(128, 128), mine[:, 1].reshape(128, 128)).T
    named, given = mine[0:4], mine[4:8]
    expert = lax.broadcasted_iota(jnp.int32, (64, 128), 0).astype(F32)
    picked = jnp.zeros((64, 128), F32)
    weight = jnp.zeros((64, 128), F32)
    for i in range(4):
        hit = named[i : i + 1, :] == expert
        picked = picked + jnp.where(hit, 1.0, 0.0)
        weight = weight + jnp.where(hit, given[i : i + 1, :], 0.0)
    r = lax.broadcasted_iota(jnp.int32, (128, 128), 0)
    t = lax.broadcasted_iota(jnp.int32, (128, 128), 1)
    earlier = jnp.where((lax.shift_right_logical(r, 4) == lax.shift_right_logical(t, 4)) & (r < t), 1.0, 0.0)
    rank = jnp.dot(picked.astype(BF), earlier.astype(BF), preferred_element_type=F32)
    slot = lax.broadcasted_iota(jnp.int32, (1, 16, 128), 1)
    to = lax.broadcasted_iota(jnp.int32, (1, 16, 128), 2)
    fits = jnp.where(lax.shift_right_logical(slot, 1) == lax.shift_right_logical(to, 4), 1.0, 0.0)
    turn = (slot & 1).astype(F32)
    shape = (64, 16, 128)
    taken = jnp.where(
        jnp.broadcast_to(rank[:, None, :], shape) == jnp.broadcast_to(turn, shape),
        jnp.broadcast_to(picked[:, None, :], shape) * jnp.broadcast_to(fits, shape),
        0.0,
    )
    DM[...] = taken.reshape(1024, 128).astype(BF)
    weighted = (taken * jnp.broadcast_to(weight[:, None, :], shape)).reshape(1024, 128).T
    high = weighted.astype(BF)
    DH[...] = high
    DL[...] = (weighted - high.astype(F32)).astype(BF)


def log_sigmoid(v):
    return jnp.minimum(v, 0.0) - jnp.log1p(jnp.exp(-jnp.abs(v)))


def cell(Mg, GB, SM, HG, SN, ST, NM, NN, NX, HO, qt, kt, vv, cc, oo, num, dn):
    step = pl.program_id(0)

    @pl.when(step == 0)
    def _():
        acc = jnp.sum(Mg[...].astype(F32), axis=0)
        ext = acc[:, 0:128] + pltpu.roll(acc[:, 0:128], 64, 1)
        inv = lax.rsqrt(ext[:, 0:1] * (1.0 / D) + EPSILON)
        proj = (acc[:, 128:] * inv).astype(BF).astype(F32)
        pre = ext * inv
        in_log = SOFT_CAP * jnp.tanh((pre + GB[3:4, :]) / SOFT_CAP)
        forget = pltpu.roll(pre, 124, 1)
        forget_log = log_sigmoid(SOFT_CAP * jnp.tanh((forget + GB[4:5, :]) / SOFT_CAP))
        smax = jnp.concatenate(
            [jnp.zeros((8, 16), F32), SM[...], jnp.zeros((116, 16), F32)], axis=0
        )
        smax = jnp.concatenate([smax, jnp.zeros((128, 112), F32)], axis=1).T[0:16]
        new_max = jnp.maximum(forget_log + smax, in_log)
        carried = jnp.exp(forget_log + smax - new_max)
        fresh = jnp.exp(in_log - new_max)
        floor = jnp.exp(-new_max)
        NX[...] = jnp.concatenate([new_max, jnp.zeros((112, 128), F32)], axis=0).T[8:12, 0:16]
        cc[...] = carried
        q = proj[:, 0:256] * 0.125
        k = proj[:, 256:512]
        vv[...] = proj[:, 512:1024]
        oo[...] = proj[:, 1024:1536]
        fk = []
        for h in range(4):
            lane = slice(8 + h, 9 + h)
            kh = k[:, h * 64 : (h + 1) * 64] * fresh[:, lane]
            qh = q[:, h * 64 : (h + 1) * 64]
            nn = carried[:, lane] * SN[:, h, :] + kh
            NN[:, h, :] = nn
            den = jnp.sum(nn * qh, axis=1, keepdims=True)
            dn[:, h * 128 : (h + 1) * 128] = jnp.broadcast_to(
                jnp.maximum(jnp.abs(den), floor[:, lane]), (16, 128)
            )
            fk.append(kh)
        fk = jnp.concatenate(fk, axis=1)
        zeros = jnp.zeros((112, 256), F32)
        qt[...] = jnp.concatenate([q, zeros], axis=0).T
        kt[...] = jnp.concatenate([fk, zeros], axis=0).T

    shift = rem(128 - step * 4, 128)
    qr = pltpu.roll(qt[...], shift, 1)
    kr = pltpu.roll(kt[...], shift, 1)
    for r in range(4):
        row = step * 4 + r
        crow = cc[pl.ds(row, 1), :]
        vrow = vv[pl.ds(row, 1), :]
        for h in range(4):
            qc = jnp.broadcast_to(qr[h * 64 : (h + 1) * 64, r : r + 1], (64, 128))
            kc = jnp.broadcast_to(kr[h * 64 : (h + 1) * 64, r : r + 1], (64, 128))
            new = crow[:, 8 + h : 9 + h] * ST[r, h] + kc * vrow[:, h * 128 : (h + 1) * 128]
            NM[r, h] = new
            num[row, :, h * 128 : (h + 1) * 128] = jnp.sum(new * qc, axis=0, keepdims=True)

    @pl.when(step == 3)
    def _():
        read = jnp.concatenate([num[i] for i in range(16)], axis=0) / dn[...]
        parts = []
        for h in range(4):
            rh = read[:, h * 128 : (h + 1) * 128]
            parts.append(
                rh * lax.rsqrt(jnp.mean(rh * rh, axis=1, keepdims=True) + EPSILON)
            )
        gain = jnp.concatenate([HG[8 + h : 9 + h, :] for h in range(4)], axis=1)
        scaled = jnp.concatenate(parts, axis=1) * gain
        HO[...] = (scaled / (1.0 + jnp.exp(-oo[...]))).astype(BF)


def run_cell(mg, vec, sm, sn, st):
    full = lambda s: pl.BlockSpec(s, lambda i: (0,) * len(s))
    state = pl.BlockSpec((4, 4, 64, 128), lambda i: (i, 0, 0, 0))
    return plain(
        cell,
        (mg, vec, sm, vec, sn, st),
        [((16, 4, 64, 128), F32), ((16, 4, 64), F32), ((4, 16), F32), ((16, 512), BF)],
        grid=(4,),
        in_specs=[
            full((8, 16, 1664)),
            full((16, 128)),
            full((4, 16)),
            full((16, 128)),
            full((16, 4, 64)),
            state,
        ],
        out_specs=[state, full((16, 4, 64)), full((4, 16)), full((16, 512))],
        scratch=[
            ((256, 128), F32),
            ((256, 128), F32),
            ((16, 512), F32),
            ((16, 128), F32),
            ((16, 512), F32),
            ((16, 1, 512), F32),
            ((16, 512), F32),
        ],
    )


def on_device(
    tokens,
    mix_gain,
    w_query,
    w_key,
    w_value,
    w_outgate,
    w_igate,
    w_fgate,
    igate_bias,
    fgate_bias,
    head_gain,
    w_mixout,
    state_matrix,
    state_norm,
    state_max,
    ffn_gain,
    dense_mix,
    w_dense_gate,
    w_dense_up,
    w_dense_down,
    routes,
    route_weights,
    w_exp_gate,
    w_exp_up,
    w_exp_down,
):
    c = rem(lax.axis_index("ep"), 2)

    def line(v, at, lane=0):
        v = v.astype(F32).reshape(-1, min(v.shape[0], 128))
        rows, lanes = v.shape
        return jnp.pad(v, ((at, 16 - at - rows), (lane, 128 - lane - lanes)))

    vec = line(mix_gain, 0) + line(ffn_gain, 1) + line(dense_mix, 2)
    vec = vec + line(igate_bias, 3, 8) + line(fgate_bias, 4, 8) + line(head_gain, 8)
    def side_by_side(arrays, axis):
        total, at, size = None, 0, sum(v.shape[axis] for v in arrays)
        for v in arrays:
            edges = [(0, 0), (0, 0)]
            edges[axis] = (at, size - at - v.shape[axis])
            at += v.shape[axis]
            v = jnp.pad(v, edges)
            total = v if total is None else total + v
        return total

    big = side_by_side(
        [
            w_query, w_key, w_value, w_outgate, w_dense_gate, w_dense_up,
            w_mixout.T, w_dense_down.T, tokens.T,
        ],
        1,
    )
    small = side_by_side([w_igate.T, w_fgate.T], 0)
    table = side_by_side([routes.T.astype(F32), route_weights.T], 0)
    W, T, S, G, TO, PR, MO, DO, DG, DM, DH, DL = plain(
        prep,
        (vec, big, small, table),
        [
            ((64, 1664), BF),
            ((8, 64, 128), BF),
            ((8, 8, 128), F32),
            ((8, 128), F32),
            ((512, 128), BF),
            ((512, 128), BF),
            ((64, 512), BF),
            ((64, 256), BF),
            ((64, 512), BF),
            ((1024, 128), BF),
            ((128, 1024), BF),
            ((128, 1024), BF),
        ],
        scratch=[((1024, 128), F32)],
    )
    Mg, GA, Pg, Dg, Mf, Df = exchange(
        project,
        (W, T, S, G, PR, DG, MO, DO),
        [
            ((8, 16, 1664), BF),
            ((8, 8, 128), F32),
            ((512, 128), BF),
            ((64, 512), BF),
            ((64, 512), BF),
            ((64, 256), BF),
        ],
        [
            ((8, 64, 1664), BF),
            ((8, 64, 128), BF),
            ((8, 8, 128), F32),
            ((8, 8, 128), F32),
            ((8, 16, 1664), BF),
            ((8, 128), F32),
        ],
        74,
        0,
    )
    new_matrix, new_norm, nx, heads = run_cell(Mg, vec, state_max.T, state_norm, state_matrix)
    new_max = nx.T
    rows, whole = ((128, 128), BF), ((8, 8, 16, 128), BF)
    (Fo,) = exchange(
        branches,
        (heads, MO, Mf, Pg, TO, GA, DG, Dg, DM, DO, Df, DH, DL, w_exp_gate, w_exp_up, w_exp_down),
        [((2, 4, 128, 128), BF)],
        [
            ((8, 4, 16, 512), BF),
            ((4, 128, 128), BF),
            ((4, 128, 128), BF),
            rows,
            ((4, 128, 128), BF),
            whole,
            whole,
            ((4, 8, 16, 640), BF),
            ((4, 8, 16, 640), BF),
            ((8, 16, 640), BF),
            ((8, 16, 640), BF),
            ((4, 8, 8, 16, 128), BF),
            ((16, 256), BF),
            ((4096, 256), BF),
            ((4096, 256), BF),
            ((256, 4096), BF),
            ((128, 256), F32),
            ((128, 256), F32),
            ((128, 128), F32),
            ((4, 8, 8, 16, 128), BF),
            ((4, 8, 8, 16, 128), BF),
            whole,
            whole,
            whole,
            ((8, 4, 16, 256), BF),
            ((4, 128, 128), BF),
            ((4, 128, 128), BF),
            rows,
        ],
        262,
        1,
        hbm=(13, 14, 15),
        limit=52000,
    )
    both = Fo.reshape(2, 32, 16, 128)
    mine = jnp.where(c == 0, both[..., :64], both[..., 64:])
    layer_out = mine.transpose(1, 0, 2, 3).reshape(1024, 64)
    return (layer_out, new_matrix, new_norm, new_max)


def solution(mesh):
    return jax.shard_map(
        on_device,
        mesh=mesh,
        in_specs=(
            P(None, "ep"),
            P("ep"),
            P("ep", "tp"),
            P("ep", "tp"),
            P("ep", "tp"),
            P("ep", "tp"),
            P("ep", "tp"),
            P("ep", "tp"),
            P("tp"),
            P("tp"),
            P("tp"),
            P("tp", "ep"),
            P("ep", "tp", None, None),
            P("ep", "tp", None),
            P("ep", "tp"),
            P("ep"),
            P("ep"),
            P("ep", "tp"),
            P("ep", "tp"),
            P("tp", "ep"),
            P(),
            P(),
            P("ep", None, "tp"),
            P("ep", None, "tp"),
            P("ep", "tp", None),
        ),
        out_specs=(P(None, "ep"), P("ep", "tp", None, None), P("ep", "tp", None), P("ep", "tp")),
        check_vma=False,
    )
```

```python
import jax
import jax.numpy as jnp
from jax import lax
from jax.experimental import pallas as pl
from jax.experimental.pallas import tpu as pltpu
from jax.sharding import PartitionSpec as P

D = 4096
EPSILON = 1e-06
SOFT_CAP = 15.0
BF, F32 = jnp.bfloat16, jnp.float32
MESH = pl.DeviceIdType.MESH


def rem(a, n):
    return lax.rem(a, jnp.int32(n))


def div(a, n):
    return lax.div(a, jnp.int32(n))


def coords():
    e, x = lax.axis_index("ep"), lax.axis_index("tp")
    return div(e, 8), div(rem(e, 8), 2), rem(e, 2), x


class Net:
    def __init__(self, ssem, rsem, lsem):
        self.ssem, self.rsem, self.lsem = ssem, rsem, lsem
        self.at, self.lat = 0, 0
        self.open = []
        self.z, self.y, self.c, self.x = coords()

    def dev(self, dz=0, dy=0, dc=0, dx=0):
        z = rem(self.z + dz, 8) if dz else self.z
        y = rem(self.y + dy, 4) if dy else self.y
        c = 1 - self.c if dc else self.c
        x = rem(self.x + dx, 4) if dx else self.x
        return {"ep": z * 8 + y * 2 + c, "tp": x}

    def enter(self, peers):
        barrier = pltpu.get_barrier_semaphore()
        for p in peers:
            pl.semaphore_signal(barrier, inc=1, device_id=self.dev(**p), device_id_type=MESH)
        pl.semaphore_wait(barrier, len(peers))

    def send(self, src, dst, **peer):
        copy = pltpu.make_async_remote_copy(
            src_ref=src,
            dst_ref=dst,
            send_sem=self.ssem.at[self.at],
            recv_sem=self.rsem.at[self.at],
            device_id=self.dev(**peer),
            device_id_type=MESH,
        )
        self.at += 1
        copy.start()
        self.open.append(copy)
        return copy

    def local(self, src, dst):
        copy = pltpu.make_async_copy(src, dst, self.lsem.at[self.lat])
        self.lat += 1
        copy.start()
        return copy

    def got(self, copy):
        copy.wait_recv()
        copy.got = True

    def flush(self):
        for copy in self.open:
            if not getattr(copy, "got", False):
                self.got(copy)

    def finish(self):
        self.flush()
        for copy in self.open:
            copy.wait_send()


def exchange(body, ins, outs, scratch, copies, cid, hbm=(), limit=16 * 1024):
    vmem, far = pl.BlockSpec(memory_space=pltpu.VMEM), pl.BlockSpec(memory_space=pltpu.HBM)
    return pl.pallas_call(
        body,
        out_shape=[jax.ShapeDtypeStruct(s, t) for s, t in outs],
        in_specs=[far if i in hbm else vmem for i in range(len(ins))],
        out_specs=[vmem] * len(outs),
        scratch_shapes=[pltpu.VMEM(s, t) for s, t in scratch]
        + [
            pltpu.SemaphoreType.DMA((copies,)),
            pltpu.SemaphoreType.DMA((copies,)),
            pltpu.SemaphoreType.DMA((16,)),
        ],
        compiler_params=pltpu.CompilerParams(
            collective_id=cid, has_side_effects=True, vmem_limit_bytes=limit * 1024
        ),
        name=body.__name__,
    )(*ins)


YC = [dict(dy=dy, dc=dc) for dy in range(4) for dc in range(2) if dy or dc]
ZS = [1, 7, 2, 6, 3, 5, 4]
ZP = [dict(dz=d) for d in ZS]
YP = [dict(dy=d) for d in (1, 3, 2)]
XP = [dict(dx=d) for d in (1, 3, 2)]


UPWARD = (0, 1, 2, 4)


def core_of(n, p):
    return 1 - n.c if p["dc"] else n.c


def project(W, T, S, G, PR, DG, MO, DO, Mg, GA, Pg, Dg, Mf, Df, Wg, Tg, Sg, Gg, M, Gz, ssem, rsem, lsem):
    n = Net(ssem, rsem, lsem)
    j = n.y * 2 + n.c
    n.enter(YC + ZP)
    small = []
    for p in YC:
        to = rem(n.y + p["dy"], 4) * 2 + core_of(n, p)
        small.append(n.send(T.at[to], Tg.at[j], **p))
        small.append(n.send(S.at[to], Sg.at[j], **p))
    spans = [pl.ds(at, size) for at, size in [(0, 384), (384, 256), (640, 256), (896, 256), (1152, 256), (1408, 256)]]
    ys, cs = [], []
    for ch in spans:
        cs.append([n.send(W.at[:, ch], Wg.at[j, :, ch], dc=1)])
        ys.append([n.send(W.at[:, ch], Wg.at[j, :, ch], **p) for p in YP])
    gs = [n.send(G, Gg.at[j], **p) for p in YC]
    for mine, there in ((PR, Pg), (DG, Dg), (MO, Mf), (DO, Df)):
        n.send(mine, there, dc=1)
    Wg[j] = W[...]
    Tg[j] = T[j]
    Sg[j] = S[j]
    Gg[j] = G[...]
    def share(i):
        for p, copy in zip(YP, ys[i]):
            n.got(copy)
            piece = Wg.at[rem(n.y + 4 - p["dy"], 4) * 2 + n.c, :, spans[i]]
            cs[i].append(n.send(piece, piece, dc=1))

    share(0)
    for copy in small:
        n.got(copy)
    a = Tg[...].reshape(512, 128).T
    for i, ch in enumerate(spans):
        if i + 1 < len(spans):
            share(i + 1)
        for copy in cs[i]:
            n.got(copy)
        w = Wg[:, :, ch].reshape(512, ch.size)
        res = jnp.dot(a, w, preferred_element_type=F32)
        if i == 0:
            ss = jnp.sum(Sg[...], axis=0)
            ext = res[:, 0:128] + jnp.concatenate([ss, jnp.zeros((120, 128), F32)], axis=0).T
            high = ext.astype(BF).astype(F32)
            ext = high + pltpu.roll(ext - high, 64, 1)
            M[:, :, 0:128] = ext.astype(BF).reshape(8, 16, 128)
            M[:, :, 128:384] = res[:, 128:].astype(BF).reshape(8, 16, 256)
        else:
            M[:, :, ch] = res.astype(BF).reshape(8, 16, ch.size)
        for d in ZS:
            n.send(M.at[rem(n.z + d, 8), :, ch], Mg.at[n.z, :, ch], dz=d)
    for copy in gs:
        n.got(copy)
    Gz[...] = jnp.sum(Gg[...], axis=0)
    for d in ZS:
        n.send(Gz, GA.at[n.z], dz=d)
    GA[n.z] = Gz[...]
    Mg[n.z] = M[n.z]
    n.finish()


class Gather:
    def __init__(self, n, src, dst):
        self.n, self.src, self.dst = n, src, dst
        self.zc = {d: n.send(src, dst.at[n.z, n.y], dz=d) for d in ZS}
        dst[n.z, n.y] = src[...]
        self.ups, self.downs = {}, {}

    def onward(self, order):
        n, dst = self.n, self.dst
        for d in order:
            there = dst.at[rem(n.z + 8 - d, 8), n.y]
            if d:
                n.got(self.zc[d])
            piece = there if d else self.src
            self.ups[d] = n.send(piece, there, dy=1)
            self.downs[d] = n.send(piece, there, dy=3)

    def across(self, order):
        n, dst = self.n, self.dst
        last = []
        for d in order:
            zs = rem(n.z + 8 - d, 8)
            if d in UPWARD:
                n.got(self.ups[d])
                piece = dst.at[zs, rem(n.y + 3, 4)]
                last.append(n.send(piece, piece, dy=1))
            else:
                n.got(self.downs[d])
                piece = dst.at[zs, rem(n.y + 1, 4)]
                last.append(n.send(piece, piece, dy=3))
        for d in order:
            n.got(self.downs[d] if d in UPWARD else self.ups[d])
        return last


class Spread(Gather):
    def onward(self, order):
        n, dst = self.n, self.dst
        self.rest = []
        for d in order:
            there = dst.at[rem(n.z + 8 - d, 8), n.y]
            if d:
                n.got(self.zc[d])
            self.rest += [n.send(there if d else self.src, there, **p) for p in YP]

    def across(self, order):
        return self.rest


def high_low_pair(v, lane):
    high = v.astype(BF).astype(F32)
    return high + pltpu.roll(v - high, 1, 1)


NT = (((1,), (1,)), ((), ()))


def branches(
    Hd, MO, MF, PG, TO, GA, DGO, DGF, DM, DO, DF, DH, DL, WGh, WUh, WDh,
    Fo,
    Hg, mx, Mx, Hq, Hx, S, A, Pd, B2, Q, Q2, Gx, Hid, WG, WU, WD, ga, ua, sq,
    O, Og, R, A2, B, Hg2, Dp, Dq, out, ssem, rsem, lsem,
):
    n = Net(ssem, rsem, lsem)
    j = n.y * 2 + n.c
    weights = [n.local(WGh.at[0], WG), n.local(WUh.at[0], WU), n.local(WDh.at[0], WD)]
    n.enter(ZP + YC + XP)
    g = Spread(n, Hd, Hg)
    g.onward([0] + ZS)
    for copy in g.across([0] + ZS):
        n.got(copy)
    first = n.c == 0

    def both(own, other):
        own, other = own[...], other[...]
        return jnp.concatenate(
            [jnp.where(first, own, other), jnp.where(first, other, own)], axis=0
        )

    mx[...] = (
        lax.dot_general(
            Hg[...].reshape(512, 512), both(MO, MF), NT, preferred_element_type=F32
        )
        .astype(BF)
        .reshape(4, 128, 128)
    )
    xs = [n.send(mx.at[rem(n.x + p["dx"], 4)], Mx.at[n.x], **p) for p in XP]
    Mx[n.x] = mx[n.x]
    own = pl.ds(pl.multiple_of(n.x * 128, 128), 128)
    token = TO[own, :].astype(F32) + PG[own, :].astype(F32)
    for copy in xs:
        n.got(copy)
    mixer = jnp.sum(Mx[...].astype(F32), axis=0).astype(BF)
    hb = (token + mixer.astype(F32)).astype(BF)
    Hq[...] = hb
    Hx[n.x] = hb
    hs = [n.send(Hq, Hx.at[n.x], **p) for p in XP]
    S[...] = jnp.dot(DM[...], hb, preferred_element_type=F32).astype(BF).reshape(8, 8, 16, 128)
    zc = {d: n.send(S.at[rem(n.z + d, 8)], A.at[n.z], dz=d) for d in ZS}
    yc, local = {}, {}

    def around(d):
        zs = rem(n.z + 8 - d, 8)
        if d:
            n.got(zc[d])
        piece = A.at[zs] if d else S.at[n.z]
        yc[d] = []
        for p in YC:
            to = rem(n.y + p["dy"], 4) * 2 + core_of(n, p)
            yc[d].append(n.send(piece.at[to], Gx.at[n.x, zs, j], **p))
        local[d] = n.local(piece.at[j], Gx.at[n.x, zs, j])

    around(0)
    around(1)
    around(7)
    for copy in hs:
        n.got(copy)
    h = Hx[...].reshape(512, 128).astype(F32)
    gain, mix = GA[n.z, pl.ds(n.y, 1), :], GA[n.z, pl.ds(n.y + 4, 1), :]
    hg = h * gain
    lane = lax.broadcasted_iota(jnp.int32, (512, 128), 1)
    stats = jnp.where(
        lane == 0,
        jnp.sum(h * h, axis=1, keepdims=True),
        jnp.where(lane == 2, jnp.sum(hg * mix, axis=1, keepdims=True), 0.0),
    )
    part = (
        jnp.dot(hg.astype(BF), both(DGO, DGF), preferred_element_type=F32)
        .astype(BF)
        .reshape(8, 4, 16, 512)
    )
    stat = high_low_pair(stats, lane).astype(BF).reshape(8, 4, 16, 128)
    for y in range(4):
        Pd[y, :, :, 0:512] = part[:, y]
        Pd[y, :, :, 512:640] = stat[:, y]
    B2[n.y] = Pd[n.y]
    ds = []
    for i, d in enumerate([None, None, None] + ZS[2:]):
        if d:
            around(d)
        ds += [n.send(Pd.at[rem(n.y + p["dy"], 4), i], B2.at[n.y, i], **p) for p in YP]
    ups = {}
    ga[...] = jnp.zeros_like(ga)
    ua[...] = jnp.zeros_like(ua)
    sq[...] = jnp.zeros_like(sq)

    def sideways(d):
        for copy in yc[d]:
            n.got(copy)
        local[d].wait()
        piece = Gx.at[n.x, rem(n.z + 8 - d, 8)]
        ups[d] = [n.send(piece, piece, **p) for p in XP]

    def expert(d):
        zs = rem(n.z + 8 - d, 8)
        for copy in ups[d]:
            n.got(copy)
        parts = []
        s2 = sq[...]
        for y in range(4):
            block = Gx[:, zs, 2 * y : 2 * y + 2].reshape(128, 128).astype(F32)
            s2 = s2 + block * block
            parts.append((block * GA[zs, y : y + 1, :]).astype(BF))
        sq[...] = s2
        rows = jnp.concatenate(parts, axis=1)
        at = pl.ds(pl.multiple_of(zs * 512, 512), 512)
        ga[...] += jnp.dot(rows, WG[at, :], preferred_element_type=F32)
        ua[...] += jnp.dot(rows, WU[at, :], preferred_element_type=F32)

    def dense_down():
        for copy in ds:
            n.got(copy)
        total = jnp.sum(B2[...].astype(F32), axis=0).reshape(128, 640)
        ext = total[:, 512:640]
        lane = lax.broadcasted_iota(jnp.int32, (128, 128), 1)
        ext = jnp.where((lane == 0) | (lane == 2), ext + pltpu.roll(ext, 127, 1), 0.0)
        Q[:, :, 0:512] = total[:, 0:512].astype(BF).reshape(8, 16, 512)
        Q[:, :, 512:640] = high_low_pair(ext, lane).astype(BF).reshape(8, 16, 128)
        Q2[n.z] = Q[n.z]
        return [n.send(Q.at[rem(n.z + d, 8)], Q2.at[n.z], dz=d) for d in ZS]

    def dense_hidden(qs):
        for copy in qs:
            n.got(copy)
        s = jnp.sum(Q2[...].astype(F32), axis=0)
        ext = s[:, 512:640]
        inv = lax.rsqrt((ext[:, 0:1] + ext[:, 1:2]) * (1.0 / D) + EPSILON)
        gate = inv * (ext[:, 2:3] + ext[:, 3:4])
        gp = s[:, 0:256] * inv
        up = s[:, 256:512] * inv
        Hid[...] = (gp / (1.0 + jnp.exp(-gp)) * up / (1.0 + jnp.exp(-gate))).astype(BF)

    order = [0] + ZS
    for i in range(12):
        if i < 8:
            sideways(order[i])
        if i == 6:
            qs = dense_down()
        if 0 <= i - 4 < 8:
            if i == 4:
                weights[0].wait()
                weights[1].wait()
            expert(order[i - 4])

    inv = lax.rsqrt(jnp.sum(sq[...], axis=1, keepdims=True) * (1.0 / D) + EPSILON)
    gp = ga[...] * inv
    hid = (gp / (1.0 + jnp.exp(-gp)) * (ua[...] * inv)).astype(BF)
    weights[2].wait()
    far = [4, 3, 5, 2, 6, 1, 7, 0]
    xo, zo = {}, {}
    for d in far:
        zt = rem(n.z + d, 8)
        at = pl.ds(pl.multiple_of(zt * 512, 512), 512)
        res = jnp.dot(hid, WD[:, at], preferred_element_type=F32).astype(BF)
        for y in range(4):
            for c in range(2):
                for x in range(4):
                    O[x, zt, 2 * y + c] = res[
                        (x * 2 + c) * 16 : (x * 2 + c + 1) * 16, y * 128 : (y + 1) * 128
                    ]
        xo[d] = [n.send(O.at[rem(n.x + p["dx"], 4), zt], Og.at[n.x, zt], **p) for p in XP]
        if d == 4:
            dense_hidden(qs)
            g = Spread(n, Hid, Hg2)

    def summed(d):
        zt = rem(n.z + d, 8)
        for copy in xo[d]:
            n.got(copy)
        acc = O[n.x, zt].astype(F32)
        for p in XP:
            acc = acc + Og[rem(n.x + p["dx"], 4), zt].astype(F32)
        R[zt] = acc.astype(BF)
        if d:
            zo[d] = n.send(R.at[zt], A2.at[n.z], dz=d)

    def back(d):
        zs = rem(n.z + 8 - d, 8)
        if d:
            n.got(zo[d])
        piece = A2.at[zs] if d else R.at[n.z]
        for p in YC:
            to = rem(n.y + p["dy"], 4) * 2 + core_of(n, p)
            n.send(piece.at[to], B.at[zs, j], **p)
        B[zs, j] = piece[j]

    summed(4)
    summed(3)
    summed(5)
    g.onward([0] + ZS)
    summed(2)
    back(4)
    summed(6)
    back(3)
    last = g.across([0] + ZS)
    summed(1)
    back(5)
    for copy in last:
        n.got(copy)
    Dp[...] = (
        lax.dot_general(
            Hg2[...].reshape(512, 256), both(DO, DF), NT, preferred_element_type=F32
        )
        .astype(BF)
        .reshape(4, 128, 128)
    )
    for p in XP:
        n.send(Dp.at[rem(n.x + p["dx"], 4)], Dq.at[n.x], **p)
    Dq[n.x] = Dp[n.x]
    summed(7)
    back(2)
    summed(0)
    back(0)
    for d in (6, 1, 7):
        back(d)
    n.flush()
    got = B[...].reshape(1024, 128)
    routed = jnp.dot(DH[...], got, preferred_element_type=F32)
    routed += jnp.dot(DL[...], got, preferred_element_type=F32)
    dense = jnp.sum(Dq[...].astype(F32), axis=0)
    out[...] = (Hq[...].astype(F32) + routed + dense).astype(BF)
    cs = [n.send(out, Fo.at[n.c, n.x], **p) for p in XP]
    n.send(out, Fo.at[n.c, n.x], dc=1)
    Fo[n.c, n.x] = out[...]
    for p, copy in zip(XP, cs):
        n.got(copy)
        piece = Fo.at[n.c, rem(n.x + 4 - p["dx"], 4)]
        n.send(piece, piece, dc=1)
    n.finish()


def plain(body, ins, outs, grid=None, in_specs=None, out_specs=None, scratch=(), sems=0, limit=16 * 1024):
    vmem = pl.BlockSpec(memory_space=pltpu.VMEM)
    kw = {}
    if grid is not None:
        kw = dict(grid=grid)
    return pl.pallas_call(
        body,
        out_shape=[jax.ShapeDtypeStruct(s, t) for s, t in outs],
        in_specs=in_specs or [vmem] * len(ins),
        out_specs=out_specs or [vmem] * len(outs),
        scratch_shapes=[pltpu.VMEM(s, t) for s, t in scratch]
        + ([pltpu.SemaphoreType.DMA((sems,))] if sems else []),
        compiler_params=pltpu.CompilerParams(vmem_limit_bytes=limit * 1024),
        name=body.__name__,
        **kw,
    )(*ins)


def prep(
    big, table,
    W, T, S, G, TO, PR, MO, DO, DG, DM, DH, DL,
    tk,
):
    z, y, c, x = coords()
    vec = table[16:32, 0:128]
    W[:, 128:1664] = big[:, 0:1536]
    DG[...] = big[:, 1536:2048]
    MO[...] = big[:, 2048:2560]
    DO[...] = big[:, 2560:2816]
    vt = jnp.concatenate([vec, jnp.zeros((112, 128), F32)], axis=0).T
    row = lax.broadcasted_iota(jnp.int32, (8, 128), 0)
    gain, mix = vec[1:2, :], vec[2:3, :]

    def half(v):
        return jnp.where(c == 0, v, pltpu.roll(v, 64, 1))

    G[...] = jnp.where(row == y, half(gain), jnp.where(row == y + 4, half(mix), 0.0))
    gates = jnp.concatenate(
        [jnp.zeros((8, 64), F32), table[8:16, 0:64], jnp.zeros((112, 64), F32)], axis=0
    )
    gates = jnp.concatenate([gates, jnp.zeros((128, 64), F32)], axis=1).T
    W[:, 0:128] = gates[0:64].astype(BF)
    for k in range(8):
        block = big[:, 2816 + k * 128 : 2944 + k * 128].astype(F32)
        tk[k * 128 : (k + 1) * 128, :] = jnp.concatenate(
            [block, jnp.zeros((64, 128), F32)], axis=0
        ).T
    grid = tk[...].reshape(8, 4, 2, 16, 128)
    even = grid[:, :, 0].reshape(512, 128)
    odd = grid[:, :, 1].reshape(512, 128)
    TO[...] = half(jnp.where(c == 0, even, odd)).astype(BF)
    PR[...] = half(jnp.where(c == 0, odd, even)).astype(BF)
    eight = tk[...].reshape(8, 8, 16, 128)
    for j in range(8):
        wide = eight[:, j].reshape(128, 128).T[0:64]
        T[j] = (wide * vt[0:64, 0:1]).astype(BF)
        S[j] = jnp.where(row == 0, jnp.sum(wide * wide, axis=0, keepdims=True), 0.0)

    mine = table[0:8, pl.ds(pl.multiple_of(x * 256, 256), 256)]
    mine = jnp.concatenate([mine, jnp.zeros((120, 256), F32)], axis=0)
    mine = jnp.concatenate([mine[:, 0:128].T, mine[:, 128:256].T], axis=0).reshape(8, 2, 16, 128)
    mine = jnp.where(c == 0, mine[:, 0].reshape(128, 128), mine[:, 1].reshape(128, 128)).T
    named, given = mine[0:4], mine[4:8]
    expert = lax.broadcasted_iota(jnp.int32, (64, 128), 0).astype(F32)
    picked = jnp.zeros((64, 128), F32)
    weight = jnp.zeros((64, 128), F32)
    for i in range(4):
        hit = named[i : i + 1, :] == expert
        picked = picked + jnp.where(hit, 1.0, 0.0)
        weight = weight + jnp.where(hit, given[i : i + 1, :], 0.0)
    r = lax.broadcasted_iota(jnp.int32, (128, 128), 0)
    t = lax.broadcasted_iota(jnp.int32, (128, 128), 1)
    earlier = jnp.where((lax.shift_right_logical(r, 4) == lax.shift_right_logical(t, 4)) & (r < t), 1.0, 0.0)
    rank = jnp.dot(picked.astype(BF), earlier.astype(BF), preferred_element_type=F32)
    slot = lax.broadcasted_iota(jnp.int32, (1, 16, 128), 1)
    to = lax.broadcasted_iota(jnp.int32, (1, 16, 128), 2)
    fits = jnp.where(lax.shift_right_logical(slot, 1) == lax.shift_right_logical(to, 4), 1.0, 0.0)
    turn = (slot & 1).astype(F32)
    shape = (64, 16, 128)
    taken = jnp.where(
        jnp.broadcast_to(rank[:, None, :], shape) == jnp.broadcast_to(turn, shape),
        jnp.broadcast_to(picked[:, None, :], shape) * jnp.broadcast_to(fits, shape),
        0.0,
    )
    DM[...] = taken.reshape(1024, 128).astype(BF)
    weighted = (taken * jnp.broadcast_to(weight[:, None, :], shape)).reshape(1024, 128).T
    high = weighted.astype(BF)
    DH[...] = high
    DL[...] = (weighted - high.astype(F32)).astype(BF)


def log_sigmoid(v):
    return jnp.minimum(v, 0.0) - jnp.log1p(jnp.exp(-jnp.abs(v)))


def cell(Mg, GB, SM, HG, SN, ST, NM, NN, NX, HO, qt, kt, vv, cc, oo, num, dn):
    step = pl.program_id(0)

    @pl.when(step == 0)
    def _():
        acc = jnp.sum(Mg[...].astype(F32), axis=0)
        ext = acc[:, 0:128] + pltpu.roll(acc[:, 0:128], 64, 1)
        inv = lax.rsqrt(ext[:, 0:1] * (1.0 / D) + EPSILON)
        proj = (acc[:, 128:] * inv).astype(BF).astype(F32)
        pre = ext * inv
        in_log = SOFT_CAP * jnp.tanh((pre + GB[3:4, :]) / SOFT_CAP)
        forget = pltpu.roll(pre, 124, 1)
        forget_log = log_sigmoid(SOFT_CAP * jnp.tanh((forget + GB[4:5, :]) / SOFT_CAP))
        smax = jnp.concatenate(
            [jnp.zeros((8, 16), F32), SM[...], jnp.zeros((116, 16), F32)], axis=0
        )
        smax = jnp.concatenate([smax, jnp.zeros((128, 112), F32)], axis=1).T[0:16]
        new_max = jnp.maximum(forget_log + smax, in_log)
        carried = jnp.exp(forget_log + smax - new_max)
        fresh = jnp.exp(in_log - new_max)
        floor = jnp.exp(-new_max)
        NX[...] = jnp.concatenate([new_max, jnp.zeros((112, 128), F32)], axis=0).T[8:12, 0:16]
        cc[...] = carried
        q = proj[:, 0:256] * 0.125
        k = proj[:, 256:512]
        vv[...] = proj[:, 512:1024]
        oo[...] = proj[:, 1024:1536]
        fk = []
        for h in range(4):
            lane = slice(8 + h, 9 + h)
            kh = k[:, h * 64 : (h + 1) * 64] * fresh[:, lane]
            qh = q[:, h * 64 : (h + 1) * 64]
            nn = carried[:, lane] * SN[:, h, :] + kh
            NN[:, h, :] = nn
            den = jnp.sum(nn * qh, axis=1, keepdims=True)
            dn[:, h * 128 : (h + 1) * 128] = jnp.broadcast_to(
                jnp.maximum(jnp.abs(den), floor[:, lane]), (16, 128)
            )
            fk.append(kh)
        fk = jnp.concatenate(fk, axis=1)
        zeros = jnp.zeros((112, 256), F32)
        qt[...] = jnp.concatenate([q, zeros], axis=0).T
        kt[...] = jnp.concatenate([fk, zeros], axis=0).T

    shift = rem(128 - step * 4, 128)
    qr = pltpu.roll(qt[...], shift, 1)
    kr = pltpu.roll(kt[...], shift, 1)
    for r in range(4):
        row = step * 4 + r
        crow = cc[pl.ds(row, 1), :]
        vrow = vv[pl.ds(row, 1), :]
        for h in range(4):
            qc = jnp.broadcast_to(qr[h * 64 : (h + 1) * 64, r : r + 1], (64, 128))
            kc = jnp.broadcast_to(kr[h * 64 : (h + 1) * 64, r : r + 1], (64, 128))
            new = crow[:, 8 + h : 9 + h] * ST[r, h] + kc * vrow[:, h * 128 : (h + 1) * 128]
            NM[r, h] = new
            num[row, :, h * 128 : (h + 1) * 128] = jnp.sum(new * qc, axis=0, keepdims=True)

    @pl.when(step == 3)
    def _():
        read = jnp.concatenate([num[i] for i in range(16)], axis=0) / dn[...]
        parts = []
        for h in range(4):
            rh = read[:, h * 128 : (h + 1) * 128]
            parts.append(
                rh * lax.rsqrt(jnp.mean(rh * rh, axis=1, keepdims=True) + EPSILON)
            )
        gain = jnp.concatenate([HG[8 + h : 9 + h, :] for h in range(4)], axis=1)
        scaled = jnp.concatenate(parts, axis=1) * gain
        HO[...] = (scaled / (1.0 + jnp.exp(-oo[...]))).astype(BF)


def run_cell(mg, vec, sm, sn, st):
    full = lambda s: pl.BlockSpec(s, lambda i: (0,) * len(s))
    state = pl.BlockSpec((4, 4, 64, 128), lambda i: (i, 0, 0, 0))
    return plain(
        cell,
        (mg, vec, sm, vec, sn, st),
        [((16, 4, 64, 128), F32), ((16, 4, 64), F32), ((4, 16), F32), ((16, 512), BF)],
        grid=(4,),
        in_specs=[
            full((8, 16, 1664)),
            pl.BlockSpec((16, 128), lambda i: (1, 0)),
            full((4, 16)),
            pl.BlockSpec((16, 128), lambda i: (1, 0)),
            full((16, 4, 64)),
            state,
        ],
        out_specs=[state, full((16, 4, 64)), full((4, 16)), full((16, 512))],
        scratch=[
            ((256, 128), F32),
            ((256, 128), F32),
            ((16, 512), F32),
            ((16, 128), F32),
            ((16, 512), F32),
            ((16, 1, 512), F32),
            ((16, 512), F32),
        ],
    )


def on_device(
    tokens,
    mix_gain,
    w_query,
    w_key,
    w_value,
    w_outgate,
    w_igate,
    w_fgate,
    igate_bias,
    fgate_bias,
    head_gain,
    w_mixout,
    state_matrix,
    state_norm,
    state_max,
    ffn_gain,
    dense_mix,
    w_dense_gate,
    w_dense_up,
    w_dense_down,
    routes,
    route_weights,
    w_exp_gate,
    w_exp_up,
    w_exp_down,
):
    c = rem(lax.axis_index("ep"), 2)

    def line(v, at, lane=0):
        v = v.astype(F32)
        if v.ndim == 1:
            v = v.reshape(-1, min(v.shape[0], 128))
        rows, lanes = v.shape
        return jnp.pad(v, ((at, 32 - at - rows), (lane, 1024 - lane - lanes)))

    table = line(mix_gain, 16) + line(ffn_gain, 17) + line(dense_mix, 18)
    table = table + line(igate_bias, 19, 8) + line(fgate_bias, 20, 8) + line(head_gain, 24)
    table = table + line(routes.T, 0) + line(route_weights.T, 4)
    table = table + line(w_igate.T, 8) + line(w_fgate.T, 12)

    def side_by_side(arrays, axis):
        total, at, size = None, 0, sum(v.shape[axis] for v in arrays)
        for v in arrays:
            edges = [(0, 0), (0, 0)]
            edges[axis] = (at, size - at - v.shape[axis])
            at += v.shape[axis]
            v = jnp.pad(v, edges)
            total = v if total is None else total + v
        return total

    big = side_by_side(
        [
            w_query, w_key, w_value, w_outgate, w_dense_gate, w_dense_up,
            w_mixout.T, w_dense_down.T, tokens.T,
        ],
        1,
    )
    W, T, S, G, TO, PR, MO, DO, DG, DM, DH, DL = plain(
        prep,
        (big, table),
        [
            ((64, 1664), BF),
            ((8, 64, 128), BF),
            ((8, 8, 128), F32),
            ((8, 128), F32),
            ((512, 128), BF),
            ((512, 128), BF),
            ((64, 512), BF),
            ((64, 256), BF),
            ((64, 512), BF),
            ((1024, 128), BF),
            ((128, 1024), BF),
            ((128, 1024), BF),
        ],
        scratch=[((1024, 128), F32)],
    )
    Mg, GA, Pg, Dg, Mf, Df = exchange(
        project,
        (W, T, S, G, PR, DG, MO, DO),
        [
            ((8, 16, 1664), BF),
            ((8, 8, 128), F32),
            ((512, 128), BF),
            ((64, 512), BF),
            ((64, 512), BF),
            ((64, 256), BF),
        ],
        [
            ((8, 64, 1664), BF),
            ((8, 64, 128), BF),
            ((8, 8, 128), F32),
            ((8, 8, 128), F32),
            ((8, 16, 1664), BF),
            ((8, 128), F32),
        ],
        116,
        0,
    )
    new_matrix, new_norm, nx, heads = run_cell(Mg, table, state_max.T, state_norm, state_matrix)
    new_max = nx.T
    rows, whole = ((128, 128), BF), ((8, 8, 16, 128), BF)
    (Fo,) = exchange(
        branches,
        (heads, MO, Mf, Pg, TO, GA, DG, Dg, DM, DO, Df, DH, DL, w_exp_gate, w_exp_up, w_exp_down),
        [((2, 4, 128, 128), BF)],
        [
            ((8, 4, 16, 512), BF),
            ((4, 128, 128), BF),
            ((4, 128, 128), BF),
            rows,
            ((4, 128, 128), BF),
            whole,
            whole,
            ((4, 8, 16, 640), BF),
            ((4, 8, 16, 640), BF),
            ((8, 16, 640), BF),
            ((8, 16, 640), BF),
            ((4, 8, 8, 16, 128), BF),
            ((16, 256), BF),
            ((4096, 256), BF),
            ((4096, 256), BF),
            ((256, 4096), BF),
            ((128, 256), F32),
            ((128, 256), F32),
            ((128, 128), F32),
            ((4, 8, 8, 16, 128), BF),
            ((4, 8, 8, 16, 128), BF),
            whole,
            whole,
            whole,
            ((8, 4, 16, 256), BF),
            ((4, 128, 128), BF),
            ((4, 128, 128), BF),
            rows,
        ],
        283,
        1,
        hbm=(13, 14, 15),
        limit=52000,
    )
    both = Fo.reshape(2, 32, 16, 128)
    mine = jnp.where(c == 0, both[..., :64], both[..., 64:])
    layer_out = mine.transpose(1, 0, 2, 3).reshape(1024, 64)
    return (layer_out, new_matrix, new_norm, new_max)


def solution(mesh):
    return jax.shard_map(
        on_device,
        mesh=mesh,
        in_specs=(
            P(None, "ep"),
            P("ep"),
            P("ep", "tp"),
            P("ep", "tp"),
            P("ep", "tp"),
            P("ep", "tp"),
            P("ep", "tp"),
            P("ep", "tp"),
            P("tp"),
            P("tp"),
            P("tp"),
            P("tp", "ep"),
            P("ep", "tp", None, None),
            P("ep", "tp", None),
            P("ep", "tp"),
            P("ep"),
            P("ep"),
            P("ep", "tp"),
            P("ep", "tp"),
            P("tp", "ep"),
            P(),
            P(),
            P("ep", None, "tp"),
            P("ep", None, "tp"),
            P("ep", "tp", None),
        ),
        out_specs=(P(None, "ep"), P("ep", "tp", None, None), P("ep", "tp", None), P("ep", "tp")),
        check_vma=False,
    )
```

```python
import jax
import jax.numpy as jnp
from jax import lax
from jax.experimental import pallas as pl
from jax.experimental.pallas import tpu as pltpu
from jax.sharding import PartitionSpec as P

D = 4096
EPSILON = 1e-06
SOFT_CAP = 15.0
BF, F32 = jnp.bfloat16, jnp.float32
MESH = pl.DeviceIdType.MESH


def rem(a, n):
    return lax.rem(a, jnp.int32(n))


def div(a, n):
    return lax.div(a, jnp.int32(n))


def coords():
    e, x = lax.axis_index("ep"), lax.axis_index("tp")
    return div(e, 8), div(rem(e, 8), 2), rem(e, 2), x


class Net:
    def __init__(self, ssem, rsem, lsem):
        self.ssem, self.rsem, self.lsem = ssem, rsem, lsem
        self.at, self.lat = 0, 0
        self.open = []
        self.z, self.y, self.c, self.x = coords()

    def dev(self, dz=0, dy=0, dc=0, dx=0):
        z = rem(self.z + dz, 8) if dz else self.z
        y = rem(self.y + dy, 4) if dy else self.y
        c = 1 - self.c if dc else self.c
        x = rem(self.x + dx, 4) if dx else self.x
        return {"ep": z * 8 + y * 2 + c, "tp": x}

    def enter(self, peers):
        barrier = pltpu.get_barrier_semaphore()
        for p in peers:
            pl.semaphore_signal(barrier, inc=1, device_id=self.dev(**p), device_id_type=MESH)
        pl.semaphore_wait(barrier, len(peers))

    def send(self, src, dst, **peer):
        copy = pltpu.make_async_remote_copy(
            src_ref=src,
            dst_ref=dst,
            send_sem=self.ssem.at[self.at],
            recv_sem=self.rsem.at[self.at],
            device_id=self.dev(**peer),
            device_id_type=MESH,
        )
        self.at += 1
        copy.start()
        self.open.append(copy)
        return copy

    def local(self, src, dst):
        copy = pltpu.make_async_copy(src, dst, self.lsem.at[self.lat])
        self.lat += 1
        copy.start()
        return copy

    def got(self, copy):
        copy.wait_recv()
        copy.got = True

    def flush(self):
        for copy in self.open:
            if not getattr(copy, "got", False):
                self.got(copy)

    def finish(self):
        self.flush()
        for copy in self.open:
            copy.wait_send()


def exchange(body, ins, outs, scratch, copies, cid, hbm=(), limit=16 * 1024):
    vmem, far = pl.BlockSpec(memory_space=pltpu.VMEM), pl.BlockSpec(memory_space=pltpu.HBM)
    return pl.pallas_call(
        body,
        out_shape=[jax.ShapeDtypeStruct(s, t) for s, t in outs],
        in_specs=[far if i in hbm else vmem for i in range(len(ins))],
        out_specs=[vmem] * len(outs),
        scratch_shapes=[pltpu.VMEM(s, t) for s, t in scratch]
        + [
            pltpu.SemaphoreType.DMA((copies,)),
            pltpu.SemaphoreType.DMA((copies,)),
            pltpu.SemaphoreType.DMA((16,)),
        ],
        compiler_params=pltpu.CompilerParams(
            collective_id=cid, has_side_effects=True, vmem_limit_bytes=limit * 1024
        ),
        name=body.__name__,
    )(*ins)


YC = [dict(dy=dy, dc=dc) for dy in range(4) for dc in range(2) if dy or dc]
ZS = [1, 7, 2, 6, 3, 5, 4]
ZP = [dict(dz=d) for d in ZS]
YP = [dict(dy=d) for d in (1, 3, 2)]
XP = [dict(dx=d) for d in (1, 3, 2)]


UPWARD = (0, 1, 2, 4)


def core_of(n, p):
    return 1 - n.c if p["dc"] else n.c


def project(W, T, S, G, PR, DG, MO, DO, Mg, GA, Pg, Dg, Mf, Df, Wg, Tg, Sg, Gg, M, Gz, ssem, rsem, lsem):
    n = Net(ssem, rsem, lsem)
    j = n.y * 2 + n.c
    n.enter(YC + ZP)
    small = []
    for p in YC:
        to = rem(n.y + p["dy"], 4) * 2 + core_of(n, p)
        small.append(n.send(T.at[to], Tg.at[j], **p))
        small.append(n.send(S.at[to], Sg.at[j], **p))
    spans = [pl.ds(at, size) for at, size in [(0, 384), (384, 256), (640, 256), (896, 256), (1152, 256), (1408, 256)]]
    ys, cs = [], []
    for ch in spans:
        cs.append([n.send(W.at[:, ch], Wg.at[j, :, ch], dc=1)])
        ys.append([n.send(W.at[:, ch], Wg.at[j, :, ch], **p) for p in YP])
    gs = [n.send(G, Gg.at[j], **p) for p in YC]
    for mine, there in ((PR, Pg), (DG, Dg), (MO, Mf), (DO, Df)):
        n.send(mine, there, dc=1)
    Wg[j] = W[...]
    Tg[j] = T[j]
    Sg[j] = S[j]
    Gg[j] = G[...]
    def share(i):
        for p, copy in zip(YP, ys[i]):
            n.got(copy)
            piece = Wg.at[rem(n.y + 4 - p["dy"], 4) * 2 + n.c, :, spans[i]]
            cs[i].append(n.send(piece, piece, dc=1))

    share(0)
    for copy in small:
        n.got(copy)
    a = Tg[...].reshape(512, 128).T
    for i, ch in enumerate(spans):
        if i + 1 < len(spans):
            share(i + 1)
        for copy in cs[i]:
            n.got(copy)
        w = Wg[:, :, ch].reshape(512, ch.size)
        res = jnp.dot(a, w, preferred_element_type=F32)
        if i == 0:
            ss = jnp.sum(Sg[...], axis=0)
            ext = res[:, 0:128] + jnp.concatenate([ss, jnp.zeros((120, 128), F32)], axis=0).T
            high = ext.astype(BF).astype(F32)
            ext = high + pltpu.roll(ext - high, 64, 1)
            M[:, :, 0:128] = ext.astype(BF).reshape(8, 16, 128)
            M[:, :, 128:384] = res[:, 128:].astype(BF).reshape(8, 16, 256)
        else:
            M[:, :, ch] = res.astype(BF).reshape(8, 16, ch.size)
        for d in ZS:
            n.send(M.at[rem(n.z + d, 8), :, ch], Mg.at[n.z, :, ch], dz=d)
    for copy in gs:
        n.got(copy)
    Gz[...] = jnp.sum(Gg[...], axis=0)
    for d in ZS:
        n.send(Gz, GA.at[n.z], dz=d)
    GA[n.z] = Gz[...]
    Mg[n.z] = M[n.z]
    n.finish()


class Gather:
    def __init__(self, n, src, dst):
        self.n, self.src, self.dst = n, src, dst
        self.zc = {d: n.send(src, dst.at[n.z, n.y], dz=d) for d in ZS}
        dst[n.z, n.y] = src[...]
        self.ups, self.downs = {}, {}

    def onward(self, order):
        n, dst = self.n, self.dst
        for d in order:
            there = dst.at[rem(n.z + 8 - d, 8), n.y]
            if d:
                n.got(self.zc[d])
            piece = there if d else self.src
            self.ups[d] = n.send(piece, there, dy=1)
            self.downs[d] = n.send(piece, there, dy=3)

    def across(self, order):
        n, dst = self.n, self.dst
        last = []
        for d in order:
            zs = rem(n.z + 8 - d, 8)
            if d in UPWARD:
                n.got(self.ups[d])
                piece = dst.at[zs, rem(n.y + 3, 4)]
                last.append(n.send(piece, piece, dy=1))
            else:
                n.got(self.downs[d])
                piece = dst.at[zs, rem(n.y + 1, 4)]
                last.append(n.send(piece, piece, dy=3))
        for d in order:
            n.got(self.downs[d] if d in UPWARD else self.ups[d])
        return last


class Spread(Gather):
    def onward(self, order):
        n, dst = self.n, self.dst
        self.rest = []
        for d in order:
            there = dst.at[rem(n.z + 8 - d, 8), n.y]
            if d:
                n.got(self.zc[d])
            self.rest += [n.send(there if d else self.src, there, **p) for p in YP]

    def across(self, order):
        return self.rest


def high_low_pair(v, lane):
    high = v.astype(BF).astype(F32)
    return high + pltpu.roll(v - high, 1, 1)


NT = (((1,), (1,)), ((), ()))


def branches(
    Hd, MO, MF, PG, TO, GA, DGO, DGF, DM, DO, DF, DH, DL, WGh, WUh, WDh,
    Fo,
    Hg, mx, Mx, Hq, Hx, S, A, Pd, B2, Q, Q2, Gx, Hid, WG, WU, WD, ga, ua, sq,
    O, Og, R, A2, B, Hg2, Dp, Dq, out, ssem, rsem, lsem,
):
    n = Net(ssem, rsem, lsem)
    j = n.y * 2 + n.c
    weights = [n.local(WGh.at[0], WG), n.local(WUh.at[0], WU), n.local(WDh.at[0], WD)]
    n.enter(ZP + YC + XP)
    g = Spread(n, Hd, Hg)
    g.onward([0] + ZS)
    for copy in g.across([0] + ZS):
        n.got(copy)
    first = n.c == 0

    def both(own, other):
        own, other = own[...], other[...]
        return jnp.concatenate(
            [jnp.where(first, own, other), jnp.where(first, other, own)], axis=0
        )

    mx[...] = (
        lax.dot_general(
            Hg[...].reshape(512, 512), both(MO, MF), NT, preferred_element_type=F32
        )
        .astype(BF)
        .reshape(4, 128, 128)
    )
    xs = [n.send(mx.at[rem(n.x + p["dx"], 4)], Mx.at[n.x], **p) for p in XP]
    Mx[n.x] = mx[n.x]
    own = pl.ds(pl.multiple_of(n.x * 128, 128), 128)
    token = TO[own, :].astype(F32) + PG[own, :].astype(F32)
    for copy in xs:
        n.got(copy)
    mixer = jnp.sum(Mx[...].astype(F32), axis=0).astype(BF)
    hb = (token + mixer.astype(F32)).astype(BF)
    Hq[...] = hb
    Hx[n.x] = hb
    hs = [n.send(Hq, Hx.at[n.x], **p) for p in XP]
    S[...] = jnp.dot(DM[...], hb, preferred_element_type=F32).astype(BF).reshape(8, 8, 16, 128)
    zc = {d: n.send(S.at[rem(n.z + d, 8)], A.at[n.z], dz=d) for d in ZS}
    yc, local = {}, {}

    def around(d):
        zs = rem(n.z + 8 - d, 8)
        if d:
            n.got(zc[d])
        piece = A.at[zs] if d else S.at[n.z]
        yc[d] = []
        for p in YC:
            to = rem(n.y + p["dy"], 4) * 2 + core_of(n, p)
            yc[d].append(n.send(piece.at[to], Gx.at[n.x, zs, j], **p))
        local[d] = n.local(piece.at[j], Gx.at[n.x, zs, j])

    around(0)
    around(1)
    around(7)
    for copy in hs:
        n.got(copy)
    h = Hx[...].reshape(512, 128).astype(F32)
    gain, mix = GA[n.z, pl.ds(n.y, 1), :], GA[n.z, pl.ds(n.y + 4, 1), :]
    hg = h * gain
    lane = lax.broadcasted_iota(jnp.int32, (512, 128), 1)
    stats = jnp.where(
        lane == 0,
        jnp.sum(h * h, axis=1, keepdims=True),
        jnp.where(lane == 2, jnp.sum(hg * mix, axis=1, keepdims=True), 0.0),
    )
    part = (
        jnp.dot(hg.astype(BF), both(DGO, DGF), preferred_element_type=F32)
        .astype(BF)
        .reshape(8, 4, 16, 512)
    )
    stat = high_low_pair(stats, lane).astype(BF).reshape(8, 4, 16, 128)
    for y in range(4):
        Pd[y, :, :, 0:512] = part[:, y]
        Pd[y, :, :, 512:640] = stat[:, y]
    ups = {}
    ga[...] = jnp.zeros_like(ga)
    ua[...] = jnp.zeros_like(ua)
    sq[...] = jnp.zeros_like(sq)

    def sideways(d):
        for copy in yc[d]:
            n.got(copy)
        local[d].wait()
        piece = Gx.at[n.x, rem(n.z + 8 - d, 8)]
        ups[d] = [n.send(piece, piece, **p) for p in XP]

    def expert(d):
        zs = rem(n.z + 8 - d, 8)
        for copy in ups[d]:
            n.got(copy)
        parts = []
        s2 = sq[...]
        for y in range(4):
            block = Gx[:, zs, 2 * y : 2 * y + 2].reshape(128, 128).astype(F32)
            s2 = s2 + block * block
            parts.append((block * GA[zs, y : y + 1, :]).astype(BF))
        sq[...] = s2
        rows = jnp.concatenate(parts, axis=1)
        at = pl.ds(pl.multiple_of(zs * 512, 512), 512)
        ga[...] += jnp.dot(rows, WG[at, :], preferred_element_type=F32)
        ua[...] += jnp.dot(rows, WU[at, :], preferred_element_type=F32)

    def dense_down():
        for copy in ds:
            n.got(copy)
        total = jnp.sum(B2[...].astype(F32), axis=0).reshape(128, 640)
        ext = total[:, 512:640]
        lane = lax.broadcasted_iota(jnp.int32, (128, 128), 1)
        ext = jnp.where((lane == 0) | (lane == 2), ext + pltpu.roll(ext, 127, 1), 0.0)
        Q[:, :, 0:512] = total[:, 0:512].astype(BF).reshape(8, 16, 512)
        Q[:, :, 512:640] = high_low_pair(ext, lane).astype(BF).reshape(8, 16, 128)
        Q2[n.z] = Q[n.z]
        return [n.send(Q.at[rem(n.z + d, 8)], Q2.at[n.z], dz=d) for d in ZS]

    def dense_hidden(qs):
        for copy in qs:
            n.got(copy)
        s = jnp.sum(Q2[...].astype(F32), axis=0)
        ext = s[:, 512:640]
        inv = lax.rsqrt((ext[:, 0:1] + ext[:, 1:2]) * (1.0 / D) + EPSILON)
        gate = inv * (ext[:, 2:3] + ext[:, 3:4])
        gp = s[:, 0:256] * inv
        up = s[:, 256:512] * inv
        Hid[...] = (gp / (1.0 + jnp.exp(-gp)) * up / (1.0 + jnp.exp(-gate))).astype(BF)

    order = [0] + ZS
    B2[n.y] = Pd[n.y]
    ds = []
    for i, d in enumerate([None, None, None] + ZS[2:]):
        if d:
            around(d)
        ds += [n.send(Pd.at[rem(n.y + p["dy"], 4), i], B2.at[n.y, i], **p) for p in YP]
        if i >= 6:
            sideways(order[i - 6])
    for i in range(12):
        if 2 <= i < 8:
            sideways(order[i])
        if i == 6:
            qs = dense_down()
        if 0 <= i - 4 < 8:
            if i == 4:
                weights[0].wait()
                weights[1].wait()
            expert(order[i - 4])

    inv = lax.rsqrt(jnp.sum(sq[...], axis=1, keepdims=True) * (1.0 / D) + EPSILON)
    gp = ga[...] * inv
    hid = (gp / (1.0 + jnp.exp(-gp)) * (ua[...] * inv)).astype(BF)
    weights[2].wait()
    far = [4, 3, 5, 2, 6, 1, 7, 0]
    xo, zo = {}, {}
    for d in far:
        zt = rem(n.z + d, 8)
        at = pl.ds(pl.multiple_of(zt * 512, 512), 512)
        res = jnp.dot(hid, WD[:, at], preferred_element_type=F32).astype(BF)
        for y in range(4):
            for c in range(2):
                for x in range(4):
                    O[x, zt, 2 * y + c] = res[
                        (x * 2 + c) * 16 : (x * 2 + c + 1) * 16, y * 128 : (y + 1) * 128
                    ]
        xo[d] = [n.send(O.at[rem(n.x + p["dx"], 4), zt], Og.at[n.x, zt], **p) for p in XP]
        if d == 4:
            dense_hidden(qs)
            g = Spread(n, Hid, Hg2)

    def summed(d):
        zt = rem(n.z + d, 8)
        for copy in xo[d]:
            n.got(copy)
        acc = O[n.x, zt].astype(F32)
        for p in XP:
            acc = acc + Og[rem(n.x + p["dx"], 4), zt].astype(F32)
        R[zt] = acc.astype(BF)
        if d:
            zo[d] = n.send(R.at[zt], A2.at[n.z], dz=d)

    def back(d):
        zs = rem(n.z + 8 - d, 8)
        if d:
            n.got(zo[d])
        piece = A2.at[zs] if d else R.at[n.z]
        for p in YC:
            to = rem(n.y + p["dy"], 4) * 2 + core_of(n, p)
            n.send(piece.at[to], B.at[zs, j], **p)
        B[zs, j] = piece[j]

    summed(4)
    summed(3)
    summed(5)
    g.onward([0] + ZS)
    summed(2)
    back(4)
    summed(6)
    back(3)
    last = g.across([0] + ZS)
    summed(1)
    back(5)
    for copy in last:
        n.got(copy)
    Dp[...] = (
        lax.dot_general(
            Hg2[...].reshape(512, 256), both(DO, DF), NT, preferred_element_type=F32
        )
        .astype(BF)
        .reshape(4, 128, 128)
    )
    for p in XP:
        n.send(Dp.at[rem(n.x + p["dx"], 4)], Dq.at[n.x], **p)
    Dq[n.x] = Dp[n.x]
    summed(7)
    back(2)
    summed(0)
    back(0)
    for d in (6, 1, 7):
        back(d)
    n.flush()
    got = B[...].reshape(1024, 128)
    routed = jnp.dot(DH[...], got, preferred_element_type=F32)
    routed += jnp.dot(DL[...], got, preferred_element_type=F32)
    dense = jnp.sum(Dq[...].astype(F32), axis=0)
    out[...] = (Hq[...].astype(F32) + routed + dense).astype(BF)
    cs = [n.send(out, Fo.at[n.c, n.x], **p) for p in XP]
    n.send(out, Fo.at[n.c, n.x], dc=1)
    Fo[n.c, n.x] = out[...]
    for p, copy in zip(XP, cs):
        n.got(copy)
        piece = Fo.at[n.c, rem(n.x + 4 - p["dx"], 4)]
        n.send(piece, piece, dc=1)
    n.finish()


def plain(body, ins, outs, grid=None, in_specs=None, out_specs=None, scratch=(), sems=0, limit=16 * 1024):
    vmem = pl.BlockSpec(memory_space=pltpu.VMEM)
    kw = {}
    if grid is not None:
        kw = dict(grid=grid)
    return pl.pallas_call(
        body,
        out_shape=[jax.ShapeDtypeStruct(s, t) for s, t in outs],
        in_specs=in_specs or [vmem] * len(ins),
        out_specs=out_specs or [vmem] * len(outs),
        scratch_shapes=[pltpu.VMEM(s, t) for s, t in scratch]
        + ([pltpu.SemaphoreType.DMA((sems,))] if sems else []),
        compiler_params=pltpu.CompilerParams(vmem_limit_bytes=limit * 1024),
        name=body.__name__,
        **kw,
    )(*ins)


def prep(
    big, table,
    W, T, S, G, TO, PR, MO, DO, DG, DM, DH, DL,
    tk,
):
    z, y, c, x = coords()
    vec = table[16:32, 0:128]
    W[:, 128:1664] = big[:, 0:1536]
    DG[...] = big[:, 1536:2048]
    MO[...] = big[:, 2048:2560]
    DO[...] = big[:, 2560:2816]
    vt = jnp.concatenate([vec, jnp.zeros((112, 128), F32)], axis=0).T
    row = lax.broadcasted_iota(jnp.int32, (8, 128), 0)
    gain, mix = vec[1:2, :], vec[2:3, :]

    def half(v):
        return jnp.where(c == 0, v, pltpu.roll(v, 64, 1))

    G[...] = jnp.where(row == y, half(gain), jnp.where(row == y + 4, half(mix), 0.0))
    gates = jnp.concatenate(
        [jnp.zeros((8, 64), F32), table[8:16, 0:64], jnp.zeros((112, 64), F32)], axis=0
    )
    gates = jnp.concatenate([gates, jnp.zeros((128, 64), F32)], axis=1).T
    W[:, 0:128] = gates[0:64].astype(BF)
    for k in range(8):
        block = big[:, 2816 + k * 128 : 2944 + k * 128].astype(F32)
        tk[k * 128 : (k + 1) * 128, :] = jnp.concatenate(
            [block, jnp.zeros((64, 128), F32)], axis=0
        ).T
    grid = tk[...].reshape(8, 4, 2, 16, 128)
    even = grid[:, :, 0].reshape(512, 128)
    odd = grid[:, :, 1].reshape(512, 128)
    TO[...] = half(jnp.where(c == 0, even, odd)).astype(BF)
    PR[...] = half(jnp.where(c == 0, odd, even)).astype(BF)
    eight = tk[...].reshape(8, 8, 16, 128)
    for j in range(8):
        wide = eight[:, j].reshape(128, 128).T[0:64]
        T[j] = (wide * vt[0:64, 0:1]).astype(BF)
        S[j] = jnp.where(row == 0, jnp.sum(wide * wide, axis=0, keepdims=True), 0.0)

    mine = table[0:8, pl.ds(pl.multiple_of(x * 256, 256), 256)]
    mine = jnp.concatenate([mine, jnp.zeros((120, 256), F32)], axis=0)
    mine = jnp.concatenate([mine[:, 0:128].T, mine[:, 128:256].T], axis=0).reshape(8, 2, 16, 128)
    mine = jnp.where(c == 0, mine[:, 0].reshape(128, 128), mine[:, 1].reshape(128, 128)).T
    named, given = mine[0:4], mine[4:8]
    expert = lax.broadcasted_iota(jnp.int32, (64, 128), 0).astype(F32)
    picked = jnp.zeros((64, 128), F32)
    weight = jnp.zeros((64, 128), F32)
    for i in range(4):
        hit = named[i : i + 1, :] == expert
        picked = picked + jnp.where(hit, 1.0, 0.0)
        weight = weight + jnp.where(hit, given[i : i + 1, :], 0.0)
    r = lax.broadcasted_iota(jnp.int32, (128, 128), 0)
    t = lax.broadcasted_iota(jnp.int32, (128, 128), 1)
    earlier = jnp.where((lax.shift_right_logical(r, 4) == lax.shift_right_logical(t, 4)) & (r < t), 1.0, 0.0)
    rank = jnp.dot(picked.astype(BF), earlier.astype(BF), preferred_element_type=F32)
    slot = lax.broadcasted_iota(jnp.int32, (1, 16, 128), 1)
    to = lax.broadcasted_iota(jnp.int32, (1, 16, 128), 2)
    fits = jnp.where(lax.shift_right_logical(slot, 1) == lax.shift_right_logical(to, 4), 1.0, 0.0)
    turn = (slot & 1).astype(F32)
    shape = (64, 16, 128)
    taken = jnp.where(
        jnp.broadcast_to(rank[:, None, :], shape) == jnp.broadcast_to(turn, shape),
        jnp.broadcast_to(picked[:, None, :], shape) * jnp.broadcast_to(fits, shape),
        0.0,
    )
    DM[...] = taken.reshape(1024, 128).astype(BF)
    weighted = (taken * jnp.broadcast_to(weight[:, None, :], shape)).reshape(1024, 128).T
    high = weighted.astype(BF)
    DH[...] = high
    DL[...] = (weighted - high.astype(F32)).astype(BF)


def log_sigmoid(v):
    return jnp.minimum(v, 0.0) - jnp.log1p(jnp.exp(-jnp.abs(v)))


def cell(Mg, GB, SM, HG, SN, ST, NM, NN, NX, HO, qt, kt, vv, cc, oo, num, dn):
    step = pl.program_id(0)

    @pl.when(step == 0)
    def _():
        acc = jnp.sum(Mg[...].astype(F32), axis=0)
        ext = acc[:, 0:128] + pltpu.roll(acc[:, 0:128], 64, 1)
        inv = lax.rsqrt(ext[:, 0:1] * (1.0 / D) + EPSILON)
        proj = (acc[:, 128:] * inv).astype(BF).astype(F32)
        pre = ext * inv
        in_log = SOFT_CAP * jnp.tanh((pre + GB[3:4, :]) / SOFT_CAP)
        forget = pltpu.roll(pre, 124, 1)
        forget_log = log_sigmoid(SOFT_CAP * jnp.tanh((forget + GB[4:5, :]) / SOFT_CAP))
        smax = jnp.concatenate(
            [jnp.zeros((8, 16), F32), SM[...], jnp.zeros((116, 16), F32)], axis=0
        )
        smax = jnp.concatenate([smax, jnp.zeros((128, 112), F32)], axis=1).T[0:16]
        new_max = jnp.maximum(forget_log + smax, in_log)
        carried = jnp.exp(forget_log + smax - new_max)
        fresh = jnp.exp(in_log - new_max)
        floor = jnp.exp(-new_max)
        NX[...] = jnp.concatenate([new_max, jnp.zeros((112, 128), F32)], axis=0).T[8:12, 0:16]
        cc[...] = carried
        q = proj[:, 0:256] * 0.125
        k = proj[:, 256:512]
        vv[...] = proj[:, 512:1024]
        oo[...] = proj[:, 1024:1536]
        fk = []
        for h in range(4):
            lane = slice(8 + h, 9 + h)
            kh = k[:, h * 64 : (h + 1) * 64] * fresh[:, lane]
            qh = q[:, h * 64 : (h + 1) * 64]
            nn = carried[:, lane] * SN[:, h, :] + kh
            NN[:, h, :] = nn
            den = jnp.sum(nn * qh, axis=1, keepdims=True)
            dn[:, h * 128 : (h + 1) * 128] = jnp.broadcast_to(
                jnp.maximum(jnp.abs(den), floor[:, lane]), (16, 128)
            )
            fk.append(kh)
        fk = jnp.concatenate(fk, axis=1)
        zeros = jnp.zeros((112, 256), F32)
        qt[...] = jnp.concatenate([q, zeros], axis=0).T
        kt[...] = jnp.concatenate([fk, zeros], axis=0).T

    shift = rem(128 - step * 4, 128)
    qr = pltpu.roll(qt[...], shift, 1)
    kr = pltpu.roll(kt[...], shift, 1)
    for r in range(4):
        row = step * 4 + r
        crow = cc[pl.ds(row, 1), :]
        vrow = vv[pl.ds(row, 1), :]
        for h in range(4):
            qc = jnp.broadcast_to(qr[h * 64 : (h + 1) * 64, r : r + 1], (64, 128))
            kc = jnp.broadcast_to(kr[h * 64 : (h + 1) * 64, r : r + 1], (64, 128))
            new = crow[:, 8 + h : 9 + h] * ST[r, h] + kc * vrow[:, h * 128 : (h + 1) * 128]
            NM[r, h] = new
            num[row, :, h * 128 : (h + 1) * 128] = jnp.sum(new * qc, axis=0, keepdims=True)

    @pl.when(step == 3)
    def _():
        read = jnp.concatenate([num[i] for i in range(16)], axis=0) / dn[...]
        parts = []
        for h in range(4):
            rh = read[:, h * 128 : (h + 1) * 128]
            parts.append(
                rh * lax.rsqrt(jnp.mean(rh * rh, axis=1, keepdims=True) + EPSILON)
            )
        gain = jnp.concatenate([HG[8 + h : 9 + h, :] for h in range(4)], axis=1)
        scaled = jnp.concatenate(parts, axis=1) * gain
        HO[...] = (scaled / (1.0 + jnp.exp(-oo[...]))).astype(BF)


def run_cell(mg, vec, sm, sn, st):
    full = lambda s: pl.BlockSpec(s, lambda i: (0,) * len(s))
    state = pl.BlockSpec((4, 4, 64, 128), lambda i: (i, 0, 0, 0))
    return plain(
        cell,
        (mg, vec, sm, vec, sn, st),
        [((16, 4, 64, 128), F32), ((16, 4, 64), F32), ((4, 16), F32), ((16, 512), BF)],
        grid=(4,),
        in_specs=[
            full((8, 16, 1664)),
            pl.BlockSpec((16, 128), lambda i: (1, 0)),
            full((4, 16)),
            pl.BlockSpec((16, 128), lambda i: (1, 0)),
            full((16, 4, 64)),
            state,
        ],
        out_specs=[state, full((16, 4, 64)), full((4, 16)), full((16, 512))],
        scratch=[
            ((256, 128), F32),
            ((256, 128), F32),
            ((16, 512), F32),
            ((16, 128), F32),
            ((16, 512), F32),
            ((16, 1, 512), F32),
            ((16, 512), F32),
        ],
    )


def on_device(
    tokens,
    mix_gain,
    w_query,
    w_key,
    w_value,
    w_outgate,
    w_igate,
    w_fgate,
    igate_bias,
    fgate_bias,
    head_gain,
    w_mixout,
    state_matrix,
    state_norm,
    state_max,
    ffn_gain,
    dense_mix,
    w_dense_gate,
    w_dense_up,
    w_dense_down,
    routes,
    route_weights,
    w_exp_gate,
    w_exp_up,
    w_exp_down,
):
    c = rem(lax.axis_index("ep"), 2)

    def line(v, at, lane=0):
        v = v.astype(F32)
        if v.ndim == 1:
            v = v.reshape(-1, min(v.shape[0], 128))
        rows, lanes = v.shape
        return jnp.pad(v, ((at, 32 - at - rows), (lane, 1024 - lane - lanes)))

    table = line(mix_gain, 16) + line(ffn_gain, 17) + line(dense_mix, 18)
    table = table + line(igate_bias, 19, 8) + line(fgate_bias, 20, 8) + line(head_gain, 24)
    table = table + line(routes.T, 0) + line(route_weights.T, 4)
    table = table + line(w_igate.T, 8) + line(w_fgate.T, 12)

    def side_by_side(arrays, axis):
        total, at, size = None, 0, sum(v.shape[axis] for v in arrays)
        for v in arrays:
            edges = [(0, 0), (0, 0)]
            edges[axis] = (at, size - at - v.shape[axis])
            at += v.shape[axis]
            v = jnp.pad(v, edges)
            total = v if total is None else total + v
        return total

    big = side_by_side(
        [
            w_query, w_key, w_value, w_outgate, w_dense_gate, w_dense_up,
            w_mixout.T, w_dense_down.T, tokens.T,
        ],
        1,
    )
    W, T, S, G, TO, PR, MO, DO, DG, DM, DH, DL = plain(
        prep,
        (big, table),
        [
            ((64, 1664), BF),
            ((8, 64, 128), BF),
            ((8, 8, 128), F32),
            ((8, 128), F32),
            ((512, 128), BF),
            ((512, 128), BF),
            ((64, 512), BF),
            ((64, 256), BF),
            ((64, 512), BF),
            ((1024, 128), BF),
            ((128, 1024), BF),
            ((128, 1024), BF),
        ],
        scratch=[((1024, 128), F32)],
    )
    Mg, GA, Pg, Dg, Mf, Df = exchange(
        project,
        (W, T, S, G, PR, DG, MO, DO),
        [
            ((8, 16, 1664), BF),
            ((8, 8, 128), F32),
            ((512, 128), BF),
            ((64, 512), BF),
            ((64, 512), BF),
            ((64, 256), BF),
        ],
        [
            ((8, 64, 1664), BF),
            ((8, 64, 128), BF),
            ((8, 8, 128), F32),
            ((8, 8, 128), F32),
            ((8, 16, 1664), BF),
            ((8, 128), F32),
        ],
        116,
        0,
    )
    new_matrix, new_norm, nx, heads = run_cell(Mg, table, state_max.T, state_norm, state_matrix)
    new_max = nx.T
    rows, whole = ((128, 128), BF), ((8, 8, 16, 128), BF)
    (Fo,) = exchange(
        branches,
        (heads, MO, Mf, Pg, TO, GA, DG, Dg, DM, DO, Df, DH, DL, w_exp_gate, w_exp_up, w_exp_down),
        [((2, 4, 128, 128), BF)],
        [
            ((8, 4, 16, 512), BF),
            ((4, 128, 128), BF),
            ((4, 128, 128), BF),
            rows,
            ((4, 128, 128), BF),
            whole,
            whole,
            ((4, 8, 16, 640), BF),
            ((4, 8, 16, 640), BF),
            ((8, 16, 640), BF),
            ((8, 16, 640), BF),
            ((4, 8, 8, 16, 128), BF),
            ((16, 256), BF),
            ((4096, 256), BF),
            ((4096, 256), BF),
            ((256, 4096), BF),
            ((128, 256), F32),
            ((128, 256), F32),
            ((128, 128), F32),
            ((4, 8, 8, 16, 128), BF),
            ((4, 8, 8, 16, 128), BF),
            whole,
            whole,
            whole,
            ((8, 4, 16, 256), BF),
            ((4, 128, 128), BF),
            ((4, 128, 128), BF),
            rows,
        ],
        283,
        1,
        hbm=(13, 14, 15),
        limit=52000,
    )
    both = Fo.reshape(2, 32, 16, 128)
    mine = jnp.where(c == 0, both[..., :64], both[..., 64:])
    layer_out = mine.transpose(1, 0, 2, 3).reshape(1024, 64)
    return (layer_out, new_matrix, new_norm, new_max)


def solution(mesh):
    return jax.shard_map(
        on_device,
        mesh=mesh,
        in_specs=(
            P(None, "ep"),
            P("ep"),
            P("ep", "tp"),
            P("ep", "tp"),
            P("ep", "tp"),
            P("ep", "tp"),
            P("ep", "tp"),
            P("ep", "tp"),
            P("tp"),
            P("tp"),
            P("tp"),
            P("tp", "ep"),
            P("ep", "tp", None, None),
            P("ep", "tp", None),
            P("ep", "tp"),
            P("ep"),
            P("ep"),
            P("ep", "tp"),
            P("ep", "tp"),
            P("tp", "ep"),
            P(),
            P(),
            P("ep", None, "tp"),
            P("ep", None, "tp"),
            P("ep", "tp", None),
        ),
        out_specs=(P(None, "ep"), P("ep", "tp", None, None), P("ep", "tp", None), P("ep", "tp")),
        check_vma=False,
    )
```
